32 devices in a mesh: sp: 8 (over z, y), tp: 4 (over x, core).
Axes of the slice: x: 2, y: 2, z: 4, core: 2. Of those that a mesh axis runs over, the one named last changes fastest.
Arguments:
- latent: bfloat16 [2048, 2048], P('sp'), may hold values from -6 to 6
- context: bfloat16 [1024, 2048], P('sp'), may hold values from -6 to 6
- condition: bfloat16 [2048], replicated, may hold values from -6 to 6
- context_condition: bfloat16 [2048], replicated, may hold values from -6 to 6
- gain_pre: float32 [2048], replicated, may hold values from 0.1 to 1.9
- gain_post: float32 [2048], replicated, may hold values from 0.1 to 1.9
- w_shift: bfloat16 [2048, 2048], P('sp', 'tp'), may hold values from -0.125 to 0.125
- w_scale: bfloat16 [2048, 2048], P('sp', 'tp'), may hold values from -0.125 to 0.125
- w_gate: bfloat16 [2048, 2048], P('sp', 'tp'), may hold values from -0.125 to 0.125
- w_query: bfloat16 [2048, 2048], P(None, 'tp'), may hold values from -0.13258252 to 0.13258252
- w_key: bfloat16 [2048, 2048], P(None, 'tp'), may hold values from -6.629126 to 6.629126
- w_value: bfloat16 [2048, 2048], P(None, 'tp'), may hold values from -0.125 to 0.125
- w_silu: bfloat16 [2048, 2048], P(None, 'tp'), may hold values from -0.125 to 0.125
- offset_bias: float32 [32, 15, 31], P('tp'), may hold values from 1.5 to 3.5
- w_out: bfloat16 [2048, 2048], P('tp'), may hold values from -0.125 to 0.125
Outputs:
- updated: bfloat16 [2048, 2048], P(('sp', 'tp'))
The draws below stay inside these ranges and needn't reach their ends.
All inputs are finite; a program needn't handle non-finite values.
Results may differ from the reference program's by a relative error of at most 0.01.
Values may be sent and summed in bfloat16 or wider, within the bound.
No kernel may reach another device: no remote copies, remote signals or barrier semaphores. Data moves between devices by JAX's collectives and lax.ppermute only.
A program may use at most 64 MiB of HBM per device.

```python
import jax
import jax.numpy as jnp
from jax import lax

D = 2048
HEADS = 32
HEAD_DIM = 64
GRID_W = 64
WIN_ROWS = 8
WIN_COLS = 16
CTX = 1024
TOKENS = 2048
N_TP = 4


def query_key_pair(key):
    base = jax.random.fold_in(key, 7)
    first, second, third = jax.random.split(base, 3)
    spread = D ** (-0.5)
    weight_query = jnp.clip(jax.random.normal(first, (D, D), jnp.float32), -6.0, 6.0) * spread
    weight_key = jnp.clip(jax.random.normal(second, (D, D), jnp.float32), -6.0, 6.0) * spread
    return (weight_query, weight_key)


def draw_w_query(key, part):
    return query_key_pair(key)[0].astype(jnp.bfloat16)


def draw_w_key(key, part):
    return query_key_pair(key)[1].astype(jnp.bfloat16)


def steps_of(key, dims, pieces, smallest, high):
    def one(dim, shards_of):
        steps = jax.random.uniform(jax.random.fold_in(jax.random.fold_in(key, 6), dim), (shards_of,), jnp.float32, smallest / len(pieces), high / len(pieces))
        return jnp.repeat(jnp.exp(steps), dims[dim] // shards_of).reshape((-1,) + (1,) * (len(dims) - dim - 1))

    factor_of = one(*pieces[0])
    for cut in pieces[1:]:
        factor_of = factor_of * one(*cut)
    return factor_of


def scatter_about(stream_key, dims, scale, reach, cuts=(), kind=jnp.bfloat16):
    factor_of = steps_of(stream_key, dims, cuts, -0.22, 0.18) if cuts else 1.0
    values = jax.random.normal(stream_key, dims, jnp.float32) * scale * factor_of
    return jnp.minimum(jnp.maximum(values, -reach), reach).astype(kind)


def setup_inputs(seed: int = 0) -> dict:
    streams_of = jax.random.split(jax.random.key(seed), 16)
    latent = scatter_about(streams_of[0], (TOKENS, D), 1.0, 6.0, ((0, 8),))
    context = scatter_about(streams_of[1], (CTX, D), 1.0, 6.0, ((0, 8),))
    condition = scatter_about(streams_of[2], (D,), 1.0, 6.0)
    context_condition = scatter_about(streams_of[3], (D,), 1.0, 6.0)
    gain_pre = jnp.clip(1.0 + 0.18 * jax.random.normal(streams_of[4], (D,), jnp.float32), 0.1, 1.9)
    gain_post = jnp.clip(1.0 + 0.18 * jax.random.normal(streams_of[5], (D,), jnp.float32), 0.1, 1.9)
    w_shift = scatter_about(streams_of[6], (D, D), D ** -0.5, 0.125, ((0, 8), (1, 4)))
    w_scale = scatter_about(streams_of[7], (D, D), D ** -0.5, 0.125, ((0, 8), (1, 4)))
    w_gate = scatter_about(streams_of[8], (D, D), D ** -0.5, 0.125, ((0, 8), (1, 4)))
    w_query = draw_w_query(jax.random.fold_in(streams_of[15], 71), 0)
    w_key = draw_w_key(jax.random.fold_in(streams_of[15], 71), 0)
    w_value = scatter_about(streams_of[11], (D, D), D ** -0.5, 0.125, ((1, 4),))
    w_silu = scatter_about(streams_of[12], (D, D), D ** -0.5, 0.125, ((1, 4),))
    offset_bias = jnp.clip(1.5 + 2.0 * jax.random.uniform(streams_of[13], (HEADS, 2 * WIN_ROWS - 1, 2 * WIN_COLS - 1), jnp.float32) ** steps_of(streams_of[13], (HEADS, 2 * WIN_ROWS - 1, 2 * WIN_COLS - 1), ((0, 4),), -0.2, 0.2), 1.5, 3.5)
    w_out = scatter_about(streams_of[14], (D, D), D ** -0.5, 0.125, ((0, 4),))
    return {"latent": latent, "context": context, "condition": condition, "context_condition": context_condition, "gain_pre": gain_pre, "gain_post": gain_post, "w_shift": w_shift, "w_scale": w_scale, "w_gate": w_gate, "w_query": w_query, "w_key": w_key, "w_value": w_value, "w_silu": w_silu, "offset_bias": offset_bias, "w_out": w_out}


EPSILON = 1e-06

def rounded(values):
    return lax.optimization_barrier(values.astype(jnp.bfloat16))

def normalize(row_block, gain_row):
    values = row_block.astype(jnp.float32)
    return values * lax.rsqrt(lax.optimization_barrier(jnp.mean(values * values, axis=-1, keepdims=True)) + EPSILON) * gain_row

def project(row_block, weight):
    return rounded(jnp.dot(row_block, weight, preferred_element_type=jnp.float32))

def reference(latent, context, condition, context_condition, gain_pre, gain_post, w_shift, w_scale, w_gate, w_query, w_key, w_value, w_silu, offset_bias, w_out):
    active = jax.nn.silu(jnp.stack([condition, context_condition]).astype(jnp.float32)).astype(jnp.bfloat16)
    shifts = jnp.dot(active, w_shift, preferred_element_type=jnp.float32)
    scales = jnp.dot(active, w_scale, preferred_element_type=jnp.float32)
    gating = jnp.dot(active, w_gate, preferred_element_type=jnp.float32)
    hidden = rounded(normalize(latent, gain_pre) * (1.0 + scales[0]) + shifts[0])
    context_hidden = rounded(normalize(context, gain_pre) * (1.0 + scales[1]) + shifts[1])
    queries = project(hidden, w_query)
    keys_latent = project(hidden, w_key)
    values_latent = project(hidden, w_value)
    silu_gate = project(hidden, w_silu)
    context_keys = project(context_hidden, w_key).reshape(-1, HEADS, HEAD_DIM).astype(jnp.float32)
    context_values = project(context_hidden, w_value).reshape(-1, HEADS, HEAD_DIM).astype(jnp.float32)
    tokens, model_width = latent.shape
    grid_rows = tokens // GRID_W
    score_scale = HEAD_DIM ** (-0.5)
    query_grid = queries.reshape(grid_rows, GRID_W, HEADS, HEAD_DIM)
    key_grid = keys_latent.reshape(grid_rows, GRID_W, HEADS, HEAD_DIM)
    value_grid = values_latent.reshape(grid_rows, GRID_W, HEADS, HEAD_DIM)
    columns = jnp.arange(GRID_W, dtype=jnp.int32)
    col_start = jnp.clip(columns - WIN_COLS // 2, 0, GRID_W - WIN_COLS)
    col_inside = (columns[None, :] >= col_start[:, None]) & (columns[None, :] < col_start[:, None] + WIN_COLS)
    col_offset = jnp.clip(columns[None, :] - columns[:, None] + WIN_COLS - 1, 0, 2 * WIN_COLS - 2)

    def row_step(row_index):
        row_first = jnp.clip(row_index - WIN_ROWS // 2, 0, grid_rows - WIN_ROWS)
        query_row = lax.dynamic_index_in_dim(query_grid, row_index, 0, keepdims=False).astype(jnp.float32)
        key_band = lax.dynamic_slice_in_dim(key_grid, row_first, WIN_ROWS, 0).astype(jnp.float32)
        value_band = lax.dynamic_slice_in_dim(value_grid, row_first, WIN_ROWS, 0).astype(jnp.float32)
        row_offset = row_first + jnp.arange(WIN_ROWS, dtype=jnp.int32) - row_index + WIN_ROWS - 1
        offset_terms = offset_bias[:, row_offset[:, None, None], col_offset[None, :, :]]
        window_scores = jnp.einsum('qhd,vkhd->hqvk', query_row, key_band) * score_scale + jnp.transpose(offset_terms, (0, 2, 1, 3))
        window_scores = jnp.where(col_inside[None, :, None, :], window_scores, -jnp.inf)
        context_scores = jnp.einsum('qhd,jhd->hqj', query_row, context_keys) * score_scale
        maximum = jnp.maximum(lax.optimization_barrier(jnp.max(window_scores, axis=(2, 3))), lax.optimization_barrier(jnp.max(context_scores, axis=2)))
        window_exp = jnp.exp(window_scores - maximum[:, :, None, None])
        context_exp = jnp.exp(context_scores - maximum[:, :, None])
        denominator = lax.optimization_barrier(jnp.sum(window_exp, axis=(2, 3))) + lax.optimization_barrier(jnp.sum(context_exp, axis=2))
        window_weights = rounded(window_exp / denominator[:, :, None, None]).astype(jnp.float32)
        context_weights = rounded(context_exp / denominator[:, :, None]).astype(jnp.float32)
        return jnp.einsum('hqvk,vkhd->qhd', window_weights, value_band) + jnp.einsum('hqj,jhd->qhd', context_weights, context_values)
    attended = lax.map(row_step, jnp.arange(grid_rows, dtype=jnp.int32)).reshape(tokens, model_width)
    gated_heads = rounded(jax.nn.silu(silu_gate.astype(jnp.float32)) * attended)
    group_width = model_width // N_TP
    branch_sum = jnp.zeros((tokens, model_width), jnp.float32)
    for group_index in range(N_TP):
        first_col = group_index * group_width
        term = jnp.dot(gated_heads[:, first_col:first_col + group_width], w_out[first_col:first_col + group_width], preferred_element_type=jnp.float32)
        branch_sum = branch_sum + rounded(term).astype(jnp.float32)
    branch = rounded(branch_sum)
    updated = latent.astype(jnp.float32) + gating[0] * normalize(branch, gain_post)
    return updated.astype(jnp.bfloat16)
```

```python
import jax
import jax.numpy as jnp
import numpy as np
from jax import lax
from jax.experimental import pallas as pl
from jax.experimental.pallas import tpu as pltpu
from jax.sharding import PartitionSpec as P

GRID_W = 64
WIN_ROWS = 8
WIN_COLS = 16
LANES = 128
HIDDEN_SCORE = -1e30

EPSILON = 1e-06


def extended_2(cells, sides, width):
    for axis, dim in sides:
        count = lax.axis_size(axis)
        ends = count - 1
        head = lax.slice_in_dim(cells, 0, width, axis=dim)
        tail = lax.slice_in_dim(cells, cells.shape[dim] - width, cells.shape[dim], axis=dim)
        cells = jnp.concatenate(
            [
                lax.ppermute(tail, axis, [(i, (i + 1) % count) for i in range(ends)]),
                cells,
                lax.ppermute(head, axis, [((i + 1) % count, i) for i in range(ends)]),
            ],
            axis=dim,
        )
    return cells


def normalize(row_block, gain_row):
    values = row_block.astype(jnp.float32)
    return (
        values * lax.rsqrt(jnp.mean(values * values, axis=-1, keepdims=True) + EPSILON) * gain_row
    )


def modulate(row_block, gain_row, shift_row, scale_row):
    return (normalize(row_block, gain_row) * (1.0 + scale_row) + shift_row).astype(jnp.bfloat16)


def product(left, right):
    return jnp.dot(left, right, preferred_element_type=jnp.float32)


def shards_by_rows(
    latent,
    context,
    condition,
    context_condition,
    gain_pre,
    gain_post,
    w_shift,
    w_scale,
    w_gate,
    w_query,
    w_key,
    w_value,
    w_silu,
    offset_bias,
    w_out,
):
    sp_index = lax.axis_index("sp")
    tp_index = lax.axis_index("tp")
    in_rows, local_cols = w_shift.shape
    tokens, model_width = latent.shape
    active = jax.nn.silu(jnp.stack([condition, context_condition]).astype(jnp.float32)).astype(
        jnp.bfloat16
    )
    own_active = lax.dynamic_slice_in_dim(active, sp_index * in_rows, in_rows, 1)
    stacked = jnp.stack([w_shift, w_scale, w_gate])
    partial_value = jnp.einsum(
        "ai,mij->maj", own_active, stacked, preferred_element_type=jnp.float32
    )
    summed = lax.psum(partial_value, "sp")
    modulation = lax.all_gather(summed, "tp", axis=2, tiled=True)
    shifts, scales, gating = (modulation[0], modulation[1], modulation[2])
    normed = modulate(context, gain_pre, shifts[1], scales[1])
    context_kv = lax.all_gather(
        jnp.concatenate([product(normed, w_key), product(normed, w_value)], axis=1).astype(
            jnp.bfloat16
        ),
        "sp",
        axis=0,
        tiled=True,
    )
    hidden = modulate(latent, gain_pre, shifts[0], scales[0])
    queries = product(hidden, w_query).astype(jnp.bfloat16)
    keys_latent = product(hidden, w_key).astype(jnp.bfloat16)
    values_latent = product(hidden, w_value).astype(jnp.bfloat16)
    silu_gate = product(hidden, w_silu).astype(jnp.bfloat16)
    head_count = offset_bias.shape[0]
    head_width = local_cols // head_count
    grid_rows = tokens // GRID_W
    kv_grid = jnp.concatenate([keys_latent, values_latent], axis=1).reshape(
        grid_rows, GRID_W, 2 * local_cols
    )
    extended = extended_2(kv_grid, (("sp", 0),), WIN_ROWS // 2)
    blocks = GRID_W // WIN_COLS
    key_span = 2 * WIN_COLS
    block_start = np.clip(np.arange(blocks) * WIN_COLS - WIN_COLS // 2, 0, GRID_W - key_span)
    query_col = np.arange(blocks)[:, None] * WIN_COLS + np.arange(WIN_COLS)[None, :]
    key_col = block_start[:, None] + np.arange(key_span)[None, :]
    window_start = np.clip(query_col - WIN_COLS // 2, 0, GRID_W - WIN_COLS)
    inside_cols = (key_col[:, None, :] >= window_start[:, :, None]) & (
        key_col[:, None, :] < window_start[:, :, None] + WIN_COLS
    )
    inside_window = np.broadcast_to(
        inside_cols[:, :, None, :], (blocks, WIN_COLS, WIN_ROWS, key_span)
    ).reshape(blocks, WIN_COLS, WIN_ROWS * key_span)[None, :, None, :, :]
    col_offset = np.clip(
        key_col[:, None, :] - query_col[:, :, None] + WIN_COLS - 1, 0, 2 * WIN_COLS - 2
    )
    col_table = (col_offset[..., None] == np.arange(2 * WIN_COLS - 1)).astype(np.float32)
    total_rows = grid_rows * lax.axis_size("sp")
    local_rows = jnp.arange(grid_rows, dtype=jnp.int32)
    global_row = sp_index * grid_rows + local_rows
    row_start = jnp.clip(global_row - WIN_ROWS // 2, 0, total_rows - WIN_ROWS)
    band_first = row_start - sp_index * grid_rows + WIN_ROWS // 2
    row_offset = (
        row_start[:, None]
        + jnp.arange(WIN_ROWS, dtype=jnp.int32)[None, :]
        - global_row[:, None]
        + WIN_ROWS
        - 1
    )
    row_table = (row_offset[..., None] == jnp.arange(2 * WIN_ROWS - 1, dtype=jnp.int32)).astype(
        jnp.float32
    )
    position = (
        band_first[:, None, None, None] + jnp.arange(WIN_ROWS, dtype=jnp.int32)[None, None, :, None]
    ) * GRID_W + jnp.asarray(key_col, jnp.int32)[None, :, None, :]
    flat_rows = extended.reshape(-1, 2 * local_cols)
    window_kv = jnp.take(flat_rows, position.reshape(-1), axis=0).reshape(
        grid_rows, blocks, WIN_ROWS * key_span, 2 * local_cols
    )
    window_keys = window_kv[..., :local_cols].reshape(
        grid_rows, blocks, WIN_ROWS * key_span, head_count, head_width
    )
    window_values = window_kv[..., local_cols:].reshape(
        grid_rows, blocks, WIN_ROWS * key_span, head_count, head_width
    )
    context_keys = context_kv[:, :local_cols].reshape(-1, head_count, head_width)
    context_values = context_kv[:, local_cols:].reshape(-1, head_count, head_width)
    query_blocks = queries.reshape(grid_rows, blocks, WIN_COLS, head_count, head_width)
    score_scale = head_width ** (-0.5)
    by_column = jnp.einsum(
        "hae,bqwe->hbqwa", offset_bias, jnp.asarray(col_table), precision=lax.Precision.HIGHEST
    )
    offset_terms = jnp.einsum(
        "rva,hbqwa->rbhqvw", row_table, by_column, precision=lax.Precision.HIGHEST
    ).reshape(grid_rows, blocks, head_count, WIN_COLS, WIN_ROWS * key_span)
    window_scores = (
        jnp.einsum(
            "rbqhd,rbkhd->rbhqk", query_blocks, window_keys, preferred_element_type=jnp.float32
        )
        * score_scale
    )
    window_scores = jnp.where(inside_window, window_scores + offset_terms, -jnp.inf)
    context_scores = (
        jnp.einsum(
            "rbqhd,khd->rbhqk", query_blocks, context_keys, preferred_element_type=jnp.float32
        )
        * score_scale
    )
    maximum = jnp.maximum(jnp.max(window_scores, axis=-1), jnp.max(context_scores, axis=-1))[
        ..., None
    ]
    window_exp = jnp.exp(window_scores - maximum)
    context_exp = jnp.exp(context_scores - maximum)
    denominator = jnp.sum(window_exp, axis=-1, keepdims=True) + jnp.sum(
        context_exp, axis=-1, keepdims=True
    )
    window_weights = (window_exp / denominator).astype(jnp.bfloat16)
    context_weights = (context_exp / denominator).astype(jnp.bfloat16)
    attended = jnp.einsum(
        "rbhqk,rbkhd->rbqhd", window_weights, window_values, preferred_element_type=jnp.float32
    )
    attended = attended + jnp.einsum(
        "rbhqk,khd->rbqhd", context_weights, context_values, preferred_element_type=jnp.float32
    )
    attended = attended.reshape(tokens, local_cols)
    gated_heads = (jax.nn.silu(silu_gate.astype(jnp.float32)) * attended).astype(jnp.bfloat16)
    out_rows = tokens // lax.axis_size("tp")
    branch = lax.psum_scatter(
        product(gated_heads, w_out).astype(jnp.bfloat16), "tp", scatter_dimension=0, tiled=True
    )
    own_rows = lax.dynamic_slice_in_dim(latent, tp_index * out_rows, out_rows, 0)
    updated = own_rows.astype(jnp.float32) + gating[0] * normalize(branch, gain_post)
    return updated.astype(jnp.bfloat16)


def whole(shape):
    return pl.BlockSpec(shape, lambda: (0,) * len(shape))


def low_half(shape):
    return lax.broadcasted_iota(jnp.int32, shape, len(shape) - 1) < LANES // 2


def swap_halves(block):
    return pltpu.roll(block, LANES // 2, len(block.shape) - 1)


def partial_kernel(active_ref, shift_ref, scale_ref, gate_ref, out_ref):
    active = active_ref[...]
    pieces = []
    for weight_ref, rows in ((shift_ref, 2), (scale_ref, 2), (gate_ref, 1)):
        terms = jnp.dot(active, weight_ref[...], preferred_element_type=jnp.float32)
        pieces += [terms[row : row + 1] for row in range(rows)]
    width = shift_ref.shape[1] // LANES
    for index, piece in enumerate(pieces):
        for lane in range(width):
            row = index * width + lane
            block = piece[:, lane * LANES : (lane + 1) * LANES]
            out_ref[:, row : row + 1, :] = jnp.broadcast_to(block[None], (out_ref.shape[0], 1, LANES))


def project_kernel(
    terms_ref,
    gain_ref,
    latent_ref,
    context_ref,
    query_hbm,
    key_hbm,
    value_hbm,
    silu_hbm,
    send_ref,
    silu_ref,
    gating_ref,
    weight_ref,
    hidden_ref,
    vectors_ref,
    semaphores,
    *,
    sp_count,
    tp_count,
):
    sources = (key_hbm, value_hbm, query_hbm, silu_hbm)
    copies = [
        pltpu.make_async_copy(source, weight_ref.at[index], semaphores.at[index])
        for index, source in enumerate(sources)
    ]
    for copy in copies:
        copy.start()
    tokens, model_width = latent_ref.shape
    context_tokens = context_ref.shape[0]
    cols = key_hbm.shape[1]
    width = cols // LANES
    for part in range(tp_count):
        total = terms_ref[part]
        for other in range(1, sp_count):
            total = total + terms_ref[other * tp_count + part]
        for index in range(5):
            for lane in range(width):
                first = part * cols + lane * LANES
                row = index * width + lane
                vectors_ref[index : index + 1, first : first + LANES] = total[row : row + 1]
    gating_ref[...] = vectors_ref[4:5, :]
    gain = gain_ref[...]
    for source, first, count, kind in (
        (context_ref, tokens, context_tokens, 1),
        (latent_ref, 0, tokens, 0),
    ):
        factor = gain * (1.0 + vectors_ref[2 + kind : 3 + kind, :])
        shift = vectors_ref[kind : kind + 1, :]
        step = 32

        def body(index, carry, source=source, first=first, factor=factor, shift=shift):
            start = pl.multiple_of(index * step, step)
            values = source[pl.ds(start, step), :].astype(jnp.float32)
            mean = jnp.sum(values * values, axis=-1, keepdims=True) * (1.0 / model_width)
            rows = values * lax.rsqrt(mean + EPSILON) * factor + shift
            hidden_ref[pl.ds(pl.multiple_of(first + start, step), step), :] = rows.astype(jnp.bfloat16)
            return carry

        lax.fori_loop(0, count // step, body, 0)
    half = tokens // 2
    copies[0].wait()
    keys = jnp.dot(hidden_ref[...], weight_ref[0], preferred_element_type=jnp.float32)
    copies[1].wait()
    values = jnp.dot(hidden_ref[...], weight_ref[1], preferred_element_type=jnp.float32)
    low = low_half((tokens + context_tokens, LANES))
    for pair in range(width):
        lanes = slice(pair * LANES, (pair + 1) * LANES)
        key, value = keys[:, lanes], values[:, lanes]
        send_ref[2 * pair, : tokens + context_tokens, :] = jnp.where(
            low, key, swap_halves(value)
        ).astype(jnp.bfloat16)
        send_ref[2 * pair + 1, : tokens + context_tokens, :] = jnp.where(
            low, swap_halves(key), value
        ).astype(jnp.bfloat16)
    copies[2].wait()
    queries = jnp.dot(hidden_ref[:tokens], weight_ref[2], preferred_element_type=jnp.float32)
    low = low_half((half, LANES))
    for pair in range(width):
        lanes = slice(pair * LANES, (pair + 1) * LANES)
        block = queries[:, lanes].astype(jnp.bfloat16).astype(jnp.float32) * (LANES // 2) ** -0.5
        top, bottom = block[:half], block[half:]
        send_ref[2 * pair, tokens + context_tokens :, :] = jnp.where(
            low, top, swap_halves(bottom)
        ).astype(jnp.bfloat16)
        send_ref[2 * pair + 1, tokens + context_tokens :, :] = jnp.where(
            low, swap_halves(top), bottom
        ).astype(jnp.bfloat16)
    copies[3].wait()
    silu_ref[...] = jnp.dot(
        hidden_ref[:tokens], weight_ref[3], preferred_element_type=jnp.float32
    ).astype(jnp.bfloat16)


def attend_kernel(
    base_ref, received_ref, out_ref, bias_ref, pairs_ref, kv_ref, ones_ref, context_ref, context_ones_ref
):
    blocks, rows, _ = received_ref.shape
    tokens = kv_ref.shape[0] // blocks
    context_tokens = context_ref.shape[0] // blocks
    grid_rows = tokens // GRID_W
    total_rows = blocks * grid_rows
    band_rows = bias_ref.shape[2] // GRID_W
    half = tokens // 2
    column = lax.broadcasted_iota(jnp.int32, (GRID_W, LANES), 0)
    lane = lax.broadcasted_iota(jnp.int32, (GRID_W, LANES), 1)
    key_column = lane % GRID_W
    first_column = jnp.clip(column - WIN_COLS // 2, 0, GRID_W - WIN_COLS)
    inside = (key_column >= first_column) & (key_column < first_column + WIN_COLS)
    for index in range(base_ref.shape[0]):
        row = jnp.broadcast_to(base_ref[index : index + 1, :], (GRID_W, LANES))
        toeplitz = pltpu.roll(row, 0, 1, stride=1, stride_axis=0)
        pairs_ref[index] = jnp.where(inside, toeplitz, HIDDEN_SCORE)
    hidden = jnp.full((GRID_W, LANES), HIDDEN_SCORE, jnp.float32)
    low = lane < LANES // 2
    for kind, block in enumerate((0, 1, blocks - 1)):
        band_first = min(max(block * grid_rows - WIN_ROWS // 2, 0), total_rows - band_rows)
        for query in range(grid_rows):
            query_row = block * grid_rows + query
            window_first = min(max(query_row - WIN_ROWS // 2, 0), total_rows - WIN_ROWS)
            for pair in range(band_rows // 2):
                key_row = band_first + 2 * pair
                valid = [
                    window_first <= key_row + side < window_first + WIN_ROWS for side in range(2)
                ]
                offset = key_row - query_row + WIN_ROWS - 1
                if not any(valid):
                    tile = hidden
                elif all(valid):
                    tile = pairs_ref[offset]
                elif valid[0]:
                    tile = jnp.where(low, pairs_ref[min(offset, 2 * WIN_ROWS - 3)], hidden) if offset <= 2 * WIN_ROWS - 3 else jnp.where(low, swap_halves(pairs_ref[offset - 1]), hidden)
                else:
                    tile = jnp.where(low, hidden, pairs_ref[offset]) if offset >= 0 else jnp.where(low, hidden, swap_halves(pairs_ref[offset + 1]))
                bias_ref[
                    kind,
                    query * GRID_W : (query + 1) * GRID_W,
                    pair * LANES : (pair + 1) * LANES,
                ] = tile
    for block in range(blocks):
        kv = received_ref[block, :tokens, :]
        kv_ref[block * tokens : (block + 1) * tokens, :] = kv
        ones_ref[block * tokens : (block + 1) * tokens, :] = jnp.where(
            low_half(kv.shape), jnp.ones_like(kv), kv
        )
        kv = received_ref[block, tokens : tokens + context_tokens, :]
        context_ref[block * context_tokens : (block + 1) * context_tokens, :] = kv
        context_ones_ref[block * context_tokens : (block + 1) * context_tokens, :] = jnp.where(
            low_half(kv.shape), jnp.ones_like(kv), kv
        )
    low_block = low_half((half, LANES))
    contract = (((1,), (1,)), ((), ()))

    def body(block, carry):
        packed = received_ref[block, tokens + context_tokens :, :].astype(jnp.float32)
        queries = jnp.concatenate(
            [jnp.where(low_block, packed, 0.0), jnp.where(low_block, swap_halves(packed), 0.0)], axis=0
        ).astype(jnp.bfloat16)
        kind = jnp.where(block == 0, 0, jnp.where(block == blocks - 1, 2, 1))
        band = jnp.clip(block * grid_rows - WIN_ROWS // 2, 0, total_rows - band_rows) * GRID_W
        band = pl.ds(pl.multiple_of(band, GRID_W), band_rows * GRID_W)
        window = (
            lax.dot_general(queries, kv_ref[band, :], contract, preferred_element_type=jnp.float32)
            + bias_ref[kind]
        )
        context = lax.dot_general(
            queries, context_ref[...], contract, preferred_element_type=jnp.float32
        )
        maximum = jnp.maximum(
            jnp.max(window, axis=-1, keepdims=True), jnp.max(context, axis=-1, keepdims=True)
        )
        sums = jnp.dot(
            jnp.exp(window - maximum).astype(jnp.bfloat16),
            ones_ref[band, :],
            preferred_element_type=jnp.float32,
        ) + jnp.dot(
            jnp.exp(context - maximum).astype(jnp.bfloat16),
            context_ones_ref[...],
            preferred_element_type=jnp.float32,
        )
        attended = sums / swap_halves(sums)
        top, bottom = attended[:half], attended[half:]
        out_ref[block] = jnp.where(low_block, swap_halves(top), bottom).astype(jnp.bfloat16)
        return carry

    lax.fori_loop(0, blocks, body, 0)


def output_kernel(attended_ref, silu_ref, weight_ref, out_ref, gated_ref):
    heads, half, _ = attended_ref.shape
    low = low_half((half, LANES))
    for pair in range(heads // 2):
        first = attended_ref[2 * pair].astype(jnp.float32)
        second = attended_ref[2 * pair + 1].astype(jnp.float32)
        lanes = slice(pair * LANES, (pair + 1) * LANES)
        for side, block in enumerate(
            (
                jnp.where(low, first, swap_halves(second)),
                jnp.where(low, swap_halves(first), second),
            )
        ):
            gate = silu_ref[side * half : (side + 1) * half, lanes].astype(jnp.float32)
            gated_ref[side * half : (side + 1) * half, lanes] = (
                gate / (1.0 + jnp.exp(-gate)) * block
            ).astype(jnp.bfloat16)
    out_ref[...] = jnp.dot(
        gated_ref[...], weight_ref[...], preferred_element_type=jnp.float32
    ).astype(jnp.bfloat16)


def finish_kernel(terms_ref, latent_ref, gating_ref, gain_ref, out_ref):
    total = terms_ref[0].astype(jnp.float32)
    for index in range(1, terms_ref.shape[0]):
        total = total + terms_ref[index].astype(jnp.float32)
    branch = total.astype(jnp.bfloat16).astype(jnp.float32)
    mean = jnp.sum(branch * branch, axis=-1, keepdims=True) * (1.0 / branch.shape[-1])
    out_ref[...] = (
        latent_ref[...].astype(jnp.float32)
        + gating_ref[...] * (branch * lax.rsqrt(mean + EPSILON)) * gain_ref[...]
    ).astype(jnp.bfloat16)


def call(kernel, name, out_shape, scratch=(), **kwargs):
    return pl.pallas_call(
        kernel,
        name=name,
        out_shape=out_shape,
        scratch_shapes=scratch,
        compiler_params=pltpu.CompilerParams(vmem_limit_bytes=56 * 2**20),
        **kwargs,
    )


def shards_by_heads(
    latent,
    context,
    condition,
    context_condition,
    gain_pre,
    gain_post,
    w_shift,
    w_scale,
    w_gate,
    w_query,
    w_key,
    w_value,
    w_silu,
    offset_bias,
    w_out,
):
    sp_index = lax.axis_index("sp")
    tp_index = lax.axis_index("tp")
    sp_count, tp_count = lax.axis_size("sp"), lax.axis_size("tp")
    in_rows, cols = w_shift.shape
    tokens, model_width = latent.shape
    context_tokens = context.shape[0]
    width = cols // LANES
    active = jax.nn.silu(
        jnp.stack(
            [
                lax.dynamic_slice_in_dim(vector, sp_index * in_rows, in_rows, 0)
                for vector in (condition, context_condition)
            ]
        ).astype(jnp.float32)
    ).astype(jnp.bfloat16)
    f32, bf16 = jnp.float32, jnp.bfloat16
    shape = jax.ShapeDtypeStruct
    devices = sp_count * tp_count
    terms = call(partial_kernel, "partial", shape((devices, 5 * width, LANES), f32))(
        active, w_shift, w_scale, w_gate
    )
    terms = lax.all_to_all(terms, ("sp", "tp"), 0, 0, tiled=True)
    rows = tokens + context_tokens + tokens // 2
    hbm = pl.BlockSpec(memory_space=pl.ANY)
    vmem = pl.BlockSpec(memory_space=pltpu.VMEM)
    send, silu_gate, gating = call(
        lambda *refs: project_kernel(*refs, sp_count=sp_count, tp_count=tp_count),
        "project",
        (
            shape((sp_count, rows, LANES), bf16),
            shape((tokens, cols), bf16),
            shape((1, model_width), f32),
        ),
        scratch=[
            pltpu.VMEM((4, model_width, cols), bf16),
            pltpu.VMEM((tokens + context_tokens, model_width), bf16),
            pltpu.VMEM((8, model_width), f32),
            pltpu.SemaphoreType.DMA((4,)),
        ],
        in_specs=[vmem] * 4 + [hbm] * 4,
    )(
        terms,
        gain_pre.reshape(1, -1),
        latent,
        context,
        w_query,
        w_key,
        w_value,
        w_silu,
    )
    received = lax.all_to_all(send, "sp", 0, 0, tiled=True)
    table = lax.dynamic_index_in_dim(offset_bias, sp_index, 0, keepdims=False)
    rows_of, cols_of = table.shape
    centre = WIN_COLS - 1
    gap = jnp.zeros((rows_of - 1, (LANES - 2 * cols_of) // 2), f32)
    base = jnp.concatenate(
        [table[:-1, centre:], gap, table[1:], gap, table[:-1, :centre]], axis=1
    )
    band_rows = 3 * WIN_ROWS // 2
    attended = call(
        attend_kernel,
        "attend",
        shape((sp_count, tokens // 2, LANES), bf16),
        scratch=[
            pltpu.VMEM((3, tokens, band_rows * GRID_W), f32),
            pltpu.VMEM((rows_of - 1, GRID_W, LANES), f32),
            pltpu.VMEM((sp_count * tokens, LANES), bf16),
            pltpu.VMEM((sp_count * tokens, LANES), bf16),
            pltpu.VMEM((sp_count * context_tokens, LANES), bf16),
            pltpu.VMEM((sp_count * context_tokens, LANES), bf16),
        ],
    )(base, received)
    attended = lax.all_to_all(attended, "sp", 0, 0, tiled=True)
    branch = call(
        output_kernel,
        "output",
        shape((tokens, model_width), bf16),
        scratch=[pltpu.VMEM((tokens, cols), bf16)],
    )(attended, silu_gate, w_out)
    out_rows = tokens // tp_count
    branch = lax.all_to_all(
        branch.reshape(tp_count, out_rows, model_width), "tp", 0, 0, tiled=True
    )
    own_rows = lax.dynamic_slice_in_dim(latent, tp_index * out_rows, out_rows, 0)
    return call(finish_kernel, "finish", shape((out_rows, model_width), bf16))(
        branch, own_rows, gating, gain_post.reshape(1, -1)
    )


def solution(mesh):
    in_specs = (
        P("sp", None),
        P("sp", None),
        P(),
        P(),
        P(),
        P(),
        P("sp", "tp"),
        P("sp", "tp"),
        P("sp", "tp"),
        P(None, "tp"),
        P(None, "tp"),
        P(None, "tp"),
        P(None, "tp"),
        P("tp", None, None),
        P("tp", None),
    )
    out_specs = P(("sp", "tp"), None)
    sp_count, tp_count = mesh.shape["sp"], mesh.shape["tp"]

    def shards(*arrays):
        heads = arrays[13].shape[0]
        head_width = arrays[6].shape[1] // heads
        grid_rows = arrays[0].shape[0] // GRID_W
        one_head_each = (
            heads == sp_count
            and sp_count >= 3
            and 2 * head_width == LANES
            and 2 * GRID_W == LANES
            and 2 * grid_rows == WIN_ROWS
        )
        return (shards_by_heads if one_head_each else shards_by_rows)(*arrays)

    return jax.shard_map(shards, mesh=mesh, in_specs=in_specs, out_specs=out_specs, check_vma=False)
```

```python
import functools

import jax
import jax.numpy as jnp
import numpy as np
from jax import lax
from jax.experimental import pallas as pl
from jax.experimental.pallas import tpu as pltpu
from jax.sharding import PartitionSpec as P


GRID_W = 64
WIN_ROWS = 8
WIN_COLS = 16
LANES = 128
HALF = LANES // 2
HIDDEN_SCORE = -1e30

EPSILON = 1e-06


def extended_2(cells, sides, width):
    for axis, dim in sides:
        count = lax.axis_size(axis)
        ends = count - 1
        head = lax.slice_in_dim(cells, 0, width, axis=dim)
        tail = lax.slice_in_dim(cells, cells.shape[dim] - width, cells.shape[dim], axis=dim)
        cells = jnp.concatenate(
            [
                lax.ppermute(tail, axis, [(i, (i + 1) % count) for i in range(ends)]),
                cells,
                lax.ppermute(head, axis, [((i + 1) % count, i) for i in range(ends)]),
            ],
            axis=dim,
        )
    return cells


def normalize(row_block, gain_row):
    values = row_block.astype(jnp.float32)
    return (
        values * lax.rsqrt(jnp.mean(values * values, axis=-1, keepdims=True) + EPSILON) * gain_row
    )


def modulate(row_block, gain_row, shift_row, scale_row):
    return (normalize(row_block, gain_row) * (1.0 + scale_row) + shift_row).astype(jnp.bfloat16)


def product(left, right):
    return jnp.dot(left, right, preferred_element_type=jnp.float32)


def shards_by_rows(
    latent,
    context,
    condition,
    context_condition,
    gain_pre,
    gain_post,
    w_shift,
    w_scale,
    w_gate,
    w_query,
    w_key,
    w_value,
    w_silu,
    offset_bias,
    w_out,
):
    sp_index = lax.axis_index("sp")
    tp_index = lax.axis_index("tp")
    in_rows, local_cols = w_shift.shape
    tokens, _ = latent.shape
    active = jax.nn.silu(jnp.stack([condition, context_condition]).astype(jnp.float32)).astype(
        jnp.bfloat16
    )
    own_active = lax.dynamic_slice_in_dim(active, sp_index * in_rows, in_rows, 1)
    stacked = jnp.stack([w_shift, w_scale, w_gate])
    partial_value = jnp.einsum(
        "ai,mij->maj", own_active, stacked, preferred_element_type=jnp.float32
    )
    summed = lax.psum(partial_value, "sp")
    modulation = lax.all_gather(summed, "tp", axis=2, tiled=True)
    shifts, scales, gating = (modulation[0], modulation[1], modulation[2])
    normed = modulate(context, gain_pre, shifts[1], scales[1])
    context_kv = lax.all_gather(
        jnp.concatenate([product(normed, w_key), product(normed, w_value)], axis=1).astype(
            jnp.bfloat16
        ),
        "sp",
        axis=0,
        tiled=True,
    )
    hidden = modulate(latent, gain_pre, shifts[0], scales[0])
    queries = product(hidden, w_query).astype(jnp.bfloat16)
    keys_latent = product(hidden, w_key).astype(jnp.bfloat16)
    values_latent = product(hidden, w_value).astype(jnp.bfloat16)
    silu_gate = product(hidden, w_silu).astype(jnp.bfloat16)
    head_count = offset_bias.shape[0]
    head_width = local_cols // head_count
    grid_rows = tokens // GRID_W
    kv_grid = jnp.concatenate([keys_latent, values_latent], axis=1).reshape(
        grid_rows, GRID_W, 2 * local_cols
    )
    extended = extended_2(kv_grid, (("sp", 0),), WIN_ROWS // 2)
    blocks = GRID_W // WIN_COLS
    key_span = 2 * WIN_COLS
    block_start = np.clip(np.arange(blocks) * WIN_COLS - WIN_COLS // 2, 0, GRID_W - key_span)
    query_col = np.arange(blocks)[:, None] * WIN_COLS + np.arange(WIN_COLS)[None, :]
    key_col = block_start[:, None] + np.arange(key_span)[None, :]
    window_start = np.clip(query_col - WIN_COLS // 2, 0, GRID_W - WIN_COLS)
    inside_cols = (key_col[:, None, :] >= window_start[:, :, None]) & (
        key_col[:, None, :] < window_start[:, :, None] + WIN_COLS
    )
    inside_window = np.broadcast_to(
        inside_cols[:, :, None, :], (blocks, WIN_COLS, WIN_ROWS, key_span)
    ).reshape(blocks, WIN_COLS, WIN_ROWS * key_span)[None, :, None, :, :]
    col_offset = np.clip(
        key_col[:, None, :] - query_col[:, :, None] + WIN_COLS - 1, 0, 2 * WIN_COLS - 2
    )
    col_table = (col_offset[..., None] == np.arange(2 * WIN_COLS - 1)).astype(np.float32)
    total_rows = grid_rows * lax.axis_size("sp")
    local_rows = jnp.arange(grid_rows, dtype=jnp.int32)
    global_row = sp_index * grid_rows + local_rows
    row_start = jnp.clip(global_row - WIN_ROWS // 2, 0, total_rows - WIN_ROWS)
    band_first = row_start - sp_index * grid_rows + WIN_ROWS // 2
    row_offset = (
        row_start[:, None]
        + jnp.arange(WIN_ROWS, dtype=jnp.int32)[None, :]
        - global_row[:, None]
        + WIN_ROWS
        - 1
    )
    row_table = (row_offset[..., None] == jnp.arange(2 * WIN_ROWS - 1, dtype=jnp.int32)).astype(
        jnp.float32
    )
    position = (
        band_first[:, None, None, None] + jnp.arange(WIN_ROWS, dtype=jnp.int32)[None, None, :, None]
    ) * GRID_W + jnp.asarray(key_col, jnp.int32)[None, :, None, :]
    flat_rows = extended.reshape(-1, 2 * local_cols)
    window_kv = jnp.take(flat_rows, position.reshape(-1), axis=0).reshape(
        grid_rows, blocks, WIN_ROWS * key_span, 2 * local_cols
    )
    window_keys = window_kv[..., :local_cols].reshape(
        grid_rows, blocks, WIN_ROWS * key_span, head_count, head_width
    )
    window_values = window_kv[..., local_cols:].reshape(
        grid_rows, blocks, WIN_ROWS * key_span, head_count, head_width
    )
    context_keys = context_kv[:, :local_cols].reshape(-1, head_count, head_width)
    context_values = context_kv[:, local_cols:].reshape(-1, head_count, head_width)
    query_blocks = queries.reshape(grid_rows, blocks, WIN_COLS, head_count, head_width)
    score_scale = head_width ** (-0.5)
    by_column = jnp.einsum(
        "hae,bqwe->hbqwa", offset_bias, jnp.asarray(col_table), precision=lax.Precision.HIGHEST
    )
    offset_terms = jnp.einsum(
        "rva,hbqwa->rbhqvw", row_table, by_column, precision=lax.Precision.HIGHEST
    ).reshape(grid_rows, blocks, head_count, WIN_COLS, WIN_ROWS * key_span)
    window_scores = (
        jnp.einsum(
            "rbqhd,rbkhd->rbhqk", query_blocks, window_keys, preferred_element_type=jnp.float32
        )
        * score_scale
    )
    window_scores = jnp.where(inside_window, window_scores + offset_terms, -jnp.inf)
    context_scores = (
        jnp.einsum(
            "rbqhd,khd->rbhqk", query_blocks, context_keys, preferred_element_type=jnp.float32
        )
        * score_scale
    )
    maximum = jnp.maximum(jnp.max(window_scores, axis=-1), jnp.max(context_scores, axis=-1))[
        ..., None
    ]
    window_exp = jnp.exp(window_scores - maximum)
    context_exp = jnp.exp(context_scores - maximum)
    denominator = jnp.sum(window_exp, axis=-1, keepdims=True) + jnp.sum(
        context_exp, axis=-1, keepdims=True
    )
    window_weights = (window_exp / denominator).astype(jnp.bfloat16)
    context_weights = (context_exp / denominator).astype(jnp.bfloat16)
    attended = jnp.einsum(
        "rbhqk,rbkhd->rbqhd", window_weights, window_values, preferred_element_type=jnp.float32
    )
    attended = attended + jnp.einsum(
        "rbhqk,khd->rbqhd", context_weights, context_values, preferred_element_type=jnp.float32
    )
    attended = attended.reshape(tokens, local_cols)
    gated_heads = (jax.nn.silu(silu_gate.astype(jnp.float32)) * attended).astype(jnp.bfloat16)
    out_rows = tokens // lax.axis_size("tp")
    branch = lax.psum_scatter(
        product(gated_heads, w_out).astype(jnp.bfloat16), "tp", scatter_dimension=0, tiled=True
    )
    own_rows = lax.dynamic_slice_in_dim(latent, tp_index * out_rows, out_rows, 0)
    updated = own_rows.astype(jnp.float32) + gating[0] * normalize(branch, gain_post)
    return updated.astype(jnp.bfloat16)


def low_half(shape):
    return lax.broadcasted_iota(jnp.int32, shape, len(shape) - 1) < HALF


def swap_halves(block):
    return pltpu.roll(block, HALF, len(block.shape) - 1)


def head_pair(first, second):
    low = low_half(first.shape)
    return (
        jnp.where(low, first, swap_halves(second)),
        jnp.where(low, swap_halves(first), second),
    )


def partial_kernel(index_ref, condition_ref, context_ref, shift_ref, scale_ref, gate_ref, out_ref, active_ref):
    rows = shift_ref.shape[0] // LANES
    for kind, source in enumerate((condition_ref, context_ref)):
        values = source[...].astype(jnp.float32)
        active_ref[kind] = values / (1.0 + jnp.exp(-values))
    own = pl.ds(index_ref[0] * rows, rows)
    vectors = [active_ref[kind, own, :].astype(jnp.bfloat16) for kind in range(2)]
    width = shift_ref.shape[1] // LANES
    row = 0
    for weight_ref, kinds in ((shift_ref, 2), (scale_ref, 2), (gate_ref, 1)):
        both = sum(
            jnp.dot(
                jnp.concatenate([vectors[kind][part : part + 1] for kind in range(2)], axis=0),
                weight_ref[part * LANES : (part + 1) * LANES, :],
                preferred_element_type=jnp.float32,
            )
            for part in range(rows)
        )
        for kind in range(kinds):
            for lane in range(width):
                block = both[kind : kind + 1, lane * LANES : (lane + 1) * LANES].astype(out_ref.dtype)
                out_ref[:, row : row + 1, :] = jnp.broadcast_to(block[None], (out_ref.shape[0], 1, LANES))
                row += 1


def norm_kernel(latent_ref, context_ref, out_ref):
    step = 32
    first = 0
    for source in (latent_ref, context_ref):

        def body(index, carry, source=source, first=first):
            start = pl.multiple_of(index * step, step)
            values = source[pl.ds(start, step), :].astype(jnp.float32)
            mean = jnp.sum(values * values, axis=-1, keepdims=True) * (1.0 / values.shape[-1])
            out_ref[pl.ds(pl.multiple_of(first + start, step), step), :] = jnp.broadcast_to(
                lax.rsqrt(mean + EPSILON), (step, LANES)
            )
            return carry

        lax.fori_loop(0, source.shape[0] // step, body, 0)
        first += source.shape[0]


def project_kernel(
    terms_ref, gain_ref, norm_ref, context_hbm, latent_hbm, key_hbm, value_hbm, query_hbm,
    send_ref, hidden_ref, gating_ref,
    context_ref, latent_ref, key_ref, value_ref, query_ref, context_hidden_ref, vectors_ref, semaphores,
    *, sp_count, tp_count
):
    pairs = (
        (context_hbm, context_ref),
        (latent_hbm, latent_ref),
        (key_hbm, key_ref),
        (value_hbm, value_ref),
        (query_hbm, query_ref),
    )
    copies = [
        pltpu.make_async_copy(source, target, semaphores.at[index])
        for index, (source, target) in enumerate(pairs)
    ]
    for copy in copies:
        copy.start()
    cols = key_ref.shape[1]
    width = cols // LANES
    for part in range(tp_count):
        total = terms_ref[part].astype(jnp.float32)
        for other in range(1, sp_count):
            total = total + terms_ref[other * tp_count + part].astype(jnp.float32)
        for index in range(5):
            for lane in range(width):
                first = part * cols + lane * LANES
                row = index * width + lane
                vectors_ref[index : index + 1, first : first + LANES] = total[row : row + 1]
    gating_ref[...] = vectors_ref[4:5, :]
    tokens = latent_ref.shape[0]
    count = context_ref.shape[0]

    def modulate_rows(source, target, first, kind):
        factor = gain_ref[...] * (1.0 + vectors_ref[2 + kind : 3 + kind, :])
        shift = vectors_ref[kind : kind + 1, :]
        step = 32

        def body(index, carry):
            start = pl.multiple_of(index * step, step)
            norm = norm_ref[pl.ds(pl.multiple_of(first + start, step), step), :][:, :1]
            rows = source[pl.ds(start, step), :].astype(jnp.float32) * norm * factor + shift
            target[pl.ds(start, step), :] = rows.astype(jnp.bfloat16)
            return carry

        lax.fori_loop(0, source.shape[0] // step, body, 0)

    def store(keys, values, first):
        for pair in range(width):
            lanes = slice(pair * LANES, (pair + 1) * LANES)
            for head, kv in enumerate(head_pair(keys[:, lanes], values[:, lanes])):
                send_ref[2 * pair + head, first : first + keys.shape[0], :] = kv.astype(jnp.bfloat16)

    copies[0].wait()
    modulate_rows(context_ref, context_hidden_ref, tokens, 1)
    copies[1].wait()
    modulate_rows(latent_ref, hidden_ref, 0, 0)
    copies[2].wait()
    context_keys = jnp.dot(context_hidden_ref[...], key_ref[...], preferred_element_type=jnp.float32)
    keys = jnp.dot(hidden_ref[...], key_ref[...], preferred_element_type=jnp.float32)
    copies[3].wait()
    values = jnp.dot(context_hidden_ref[...], value_ref[...], preferred_element_type=jnp.float32)
    store(context_keys, values, tokens)
    values = jnp.dot(hidden_ref[...], value_ref[...], preferred_element_type=jnp.float32)
    store(keys, values, 0)
    copies[4].wait()
    queries = jnp.dot(hidden_ref[...], query_ref[...], preferred_element_type=jnp.float32)
    half = tokens // 2
    for pair in range(width):
        lanes = slice(pair * LANES, (pair + 1) * LANES)
        block = queries[:, lanes].astype(jnp.bfloat16).astype(jnp.float32) * HALF**-0.5
        for head, packed in enumerate(head_pair(block[:half], block[half:])):
            send_ref[2 * pair + head, tokens + count :, :] = packed.astype(jnp.bfloat16)


def gate_kernel(index_ref, hidden_ref, weight_ref, *out_refs):
    *out_refs, rows_ref = out_refs
    rows_ref[...] = jnp.dot(hidden_ref[...], weight_ref[...], preferred_element_type=jnp.float32)
    for offset, out_ref in enumerate(out_refs):
        count = out_ref.shape[0]
        first = pl.multiple_of((index_ref[1] ^ offset) * count, count)
        out_ref[...] = rows_ref[pl.ds(first, count), :].astype(jnp.bfloat16)


def bias_kernel(base_ref, pairs_ref):
    column = lax.broadcasted_iota(jnp.int32, (GRID_W, LANES), 0)
    key_column = lax.broadcasted_iota(jnp.int32, (GRID_W, LANES), 1) % GRID_W
    first_column = jnp.clip(column - WIN_COLS // 2, 0, GRID_W - WIN_COLS)
    inside = (key_column >= first_column) & (key_column < first_column + WIN_COLS)
    for index in range(base_ref.shape[0]):
        row = jnp.broadcast_to(base_ref[index : index + 1, :], (GRID_W, LANES))
        toeplitz = pltpu.roll(row, 0, 1, stride=1, stride_axis=0)
        pairs_ref[index] = jnp.where(inside, toeplitz, HIDDEN_SCORE)


def fill_bias(bias_ref, pairs_ref, block, blocks):
    tokens, band = bias_ref.shape
    grid_rows, band_rows = tokens // GRID_W, band // GRID_W
    total_rows = blocks * grid_rows
    hidden = jnp.full((GRID_W, LANES), HIDDEN_SCORE, jnp.float32)
    low = low_half(hidden.shape)
    last = pairs_ref.shape[0] - 1
    band_first = min(max(block * grid_rows - WIN_ROWS // 2, 0), total_rows - band_rows)
    for query in range(grid_rows):
        query_row = block * grid_rows + query
        window_first = min(max(query_row - WIN_ROWS // 2, 0), total_rows - WIN_ROWS)
        for pair in range(band_rows // 2):
            key_row = band_first + 2 * pair
            valid = [window_first <= key_row + side < window_first + WIN_ROWS for side in range(2)]
            offset = key_row - query_row + WIN_ROWS - 1
            if not any(valid):
                tile = hidden
            elif 0 <= offset <= last:
                tile = pairs_ref[offset]
            else:
                tile = swap_halves(pairs_ref[last if offset > last else 0])
            if any(valid) and not all(valid):
                tile = jnp.where(low if valid[0] else ~low, tile, hidden)
            bias_ref[
                query * GRID_W : (query + 1) * GRID_W, pair * LANES : (pair + 1) * LANES
            ] = tile


def with_ones(kv):
    return jnp.where(low_half(kv.shape), jnp.ones_like(kv), kv)


CONTRACT_LANES = (((1,), (1,)), ((), ()))


def attend_kernel(
    received_ref, pairs_ref, out_ref, kv_ref, ones_ref, context_ref, context_ones_ref, query_ref, bias_ref
):
    blocks = received_ref.shape[0]
    tokens = kv_ref.shape[0] // blocks
    context_tokens = context_ref.shape[0] // blocks
    grid_rows = tokens // GRID_W
    total_rows = blocks * grid_rows
    band_rows = bias_ref.shape[1] // GRID_W
    parts = out_ref.shape[0] // blocks
    chunk = tokens // parts
    half = tokens // 2
    for block in range(blocks):
        for first, count, values_ref, values_ones_ref in (
            (0, tokens, kv_ref, ones_ref),
            (tokens, context_tokens, context_ref, context_ones_ref),
        ):
            kv = received_ref[block, first : first + count, :]
            values_ref[block * count : (block + 1) * count, :] = kv
            values_ones_ref[block * count : (block + 1) * count, :] = with_ones(kv)
        packed = received_ref[block, tokens + context_tokens :, :].astype(jnp.float32)
        low = low_half(packed.shape)
        query_ref[block, :half, :] = jnp.where(low, packed, 0.0).astype(jnp.bfloat16)
        query_ref[block, half:, :] = jnp.where(low, swap_halves(packed), 0.0).astype(jnp.bfloat16)
    low = low_half((chunk // 2, LANES))

    def body(block, carry):
        for known in (0, 1, blocks - 1):
            pl.when(block == known)(
                functools.partial(fill_bias, bias_ref, pairs_ref, known, blocks)
            )
        band = jnp.clip(block * grid_rows - WIN_ROWS // 2, 0, total_rows - band_rows) * GRID_W
        band = pl.ds(pl.multiple_of(band, GRID_W), band_rows * GRID_W)
        queries = query_ref[block]
        context = lax.dot_general(
            queries, context_ref[...], CONTRACT_LANES, preferred_element_type=jnp.float32
        )
        window = (
            lax.dot_general(
                queries, kv_ref[band, :], CONTRACT_LANES, preferred_element_type=jnp.float32
            )
            + bias_ref[...]
        )
        maximum = jnp.maximum(
            jnp.max(window, axis=-1, keepdims=True), jnp.max(context, axis=-1, keepdims=True)
        )
        sums = jnp.dot(
            jnp.exp(context - maximum).astype(jnp.bfloat16),
            context_ones_ref[...],
            preferred_element_type=jnp.float32,
        ) + jnp.dot(
            jnp.exp(window - maximum).astype(jnp.bfloat16),
            ones_ref[band, :],
            preferred_element_type=jnp.float32,
        )
        attended = sums / swap_halves(sums)
        for part in range(parts):
            rows = attended[part * chunk : (part + 1) * chunk]
            out_ref[block * parts + part] = jnp.where(
                low, swap_halves(rows[: chunk // 2]), rows[chunk // 2 :]
            ).astype(jnp.bfloat16)
        return carry

    lax.fori_loop(0, blocks, body, 0)


def output_kernel(
    index_ref, attended_ref, latent_ref, gating_ref, gain_ref, *refs, sp_count, tp_count
):
    gate_refs, sources = refs[:tp_count], refs[tp_count : 2 * tp_count]
    out_ref, gated_ref, weight_ref, semaphores = refs[2 * tp_count :]
    copies = [
        pltpu.make_async_copy(source, weight_ref.at[index], semaphores.at[index])
        for index, source in enumerate(sources)
    ]
    for copy in copies:
        copy.start()
    half = attended_ref.shape[1]
    total = None
    for offset, copy in enumerate(copies):
        group = index_ref[1] ^ offset
        for pair in range(sp_count // 2):
            first = attended_ref[2 * pair * tp_count + group].astype(jnp.float32)
            second = attended_ref[(2 * pair + 1) * tp_count + group].astype(jnp.float32)
            lanes = slice(pair * LANES, (pair + 1) * LANES)
            for side, block in enumerate(head_pair(first, second)):
                gate = gate_refs[offset][side * half : (side + 1) * half, lanes].astype(jnp.float32)
                gated_ref[offset, side * half : (side + 1) * half, lanes] = (
                    gate / (1.0 + jnp.exp(-gate)) * block
                ).astype(jnp.bfloat16)
        copy.wait()
        term = jnp.dot(gated_ref[offset], weight_ref[offset], preferred_element_type=jnp.float32)
        total = term if total is None else total + term
    branch = total.astype(jnp.bfloat16).astype(jnp.float32)
    mean = jnp.sum(branch * branch, axis=-1, keepdims=True) * (1.0 / branch.shape[-1])
    out_ref[...] = (
        latent_ref[...].astype(jnp.float32)
        + gating_ref[...] * (branch * lax.rsqrt(mean + EPSILON)) * gain_ref[...]
    ).astype(jnp.bfloat16)


def in_vmem(array):
    return pltpu.with_memory_space_constraint(array, pltpu.VMEM)


def call(kernel, out_shape, operands, scratch=(), scalars=0, raw=0, flops=0, mib=58):
    vmem = pl.BlockSpec()
    smem, hbm = pl.BlockSpec(memory_space=pltpu.SMEM), pl.BlockSpec(memory_space=pl.ANY)
    return pl.pallas_call(
        kernel,
        in_specs=[smem] * scalars + [vmem] * (len(operands) - scalars - raw) + [hbm] * raw,
        out_specs=jax.tree.map(lambda _: vmem, out_shape),
        out_shape=out_shape,
        scratch_shapes=scratch,
        cost_estimate=pl.CostEstimate(flops=flops, transcendentals=0, bytes_accessed=0),
        compiler_params=pltpu.CompilerParams(vmem_limit_bytes=mib * 2**20),
    )(*operands)


def shards_by_heads(
    latent,
    context,
    condition,
    context_condition,
    gain_pre,
    gain_post,
    w_shift,
    w_scale,
    w_gate,
    w_query,
    w_key,
    w_value,
    w_silu,
    offset_bias,
    w_out,
):
    sp_index = lax.axis_index("sp")
    tp_index = lax.axis_index("tp")
    sp_count, tp_count = lax.axis_size("sp"), lax.axis_size("tp")
    indices = jnp.stack([sp_index, tp_index]).astype(jnp.int32)
    cols = w_shift.shape[1]
    tokens, model_width = latent.shape
    context_tokens = context.shape[0]
    rows = tokens + context_tokens
    width = cols // LANES
    f32, bf16 = jnp.float32, jnp.bfloat16
    vmem = pltpu.VMEM

    shape = jax.ShapeDtypeStruct
    across = [(index, index ^ (tp_count // 2)) for index in range(tp_count)]
    beside = [(index, index ^ 1) for index in range(tp_count)]
    dma = pltpu.SemaphoreType.DMA

    terms = call(
        partial_kernel,
        shape((sp_count * tp_count, 5 * width, LANES), bf16),
        (
            indices,
            condition.reshape(-1, LANES),
            context_condition.reshape(-1, LANES),
            w_shift,
            w_scale,
            w_gate,
        ),
        scratch=[vmem((2, model_width // LANES, LANES), f32)],
        scalars=1,
    )
    terms = lax.all_to_all(terms, ("sp", "tp"), 0, 0, tiled=True)
    far = lax.ppermute(w_out, "tp", across)
    near = lax.ppermute(w_out, "tp", beside)
    norm = call(norm_kernel, shape((rows, LANES), f32), (latent, context), flops=3 * 10**9)
    table = lax.dynamic_index_in_dim(offset_bias, sp_index, 0, keepdims=False)
    rows_of, cols_of = table.shape
    centre = WIN_COLS - 1
    gap = jnp.zeros((rows_of - 1, (LANES - 2 * cols_of) // 2), f32)
    base = jnp.concatenate([table[:-1, centre:], gap, table[1:], gap, table[:-1, :centre]], axis=1)
    pairs = call(bias_kernel, shape((rows_of - 1, GRID_W, LANES), f32), (base,), flops=3 * 10**9)
    send, hidden, gating = call(
        functools.partial(project_kernel, sp_count=sp_count, tp_count=tp_count),
        (
            shape((sp_count, rows + tokens // 2, LANES), bf16),
            shape((tokens, model_width), bf16),
            shape((1, model_width), f32),
        ),
        (in_vmem(terms), gain_pre.reshape(1, -1), norm, context, latent, w_key, w_value, w_query),
        raw=5,
        scratch=[
            vmem((context_tokens, model_width), bf16),
            vmem((tokens, model_width), bf16),
            vmem(w_key.shape, bf16),
            vmem(w_value.shape, bf16),
            vmem(w_query.shape, bf16),
            vmem((context_tokens, model_width), bf16),
            vmem((8, model_width), f32),
            dma((5,)),
        ],
        flops=10**9,
    )
    received = lax.all_to_all(send, "sp", 0, 0, tiled=True)
    out_rows = tokens // tp_count
    gates = call(
        gate_kernel,
        (shape((out_rows, cols), bf16),) * tp_count,
        (indices, hidden, w_silu),
        scratch=[vmem((tokens, cols), f32)],
        scalars=1,
        flops=10**9,
    )
    gates = [gates[0]] + [
        lax.ppermute(gates[offset], "tp", [(index, index ^ offset) for index in range(tp_count)])
        for offset in range(1, tp_count)
    ]
    relayed = lax.ppermute(far, "tp", beside)
    attended = call(
        attend_kernel,
        shape((sp_count * tp_count, out_rows // 2, LANES), bf16),
        (in_vmem(received), pairs),
        scratch=[
            vmem((sp_count * tokens, LANES), bf16),
            vmem((sp_count * tokens, LANES), bf16),
            vmem((sp_count * context_tokens, LANES), bf16),
            vmem((sp_count * context_tokens, LANES), bf16),
            vmem((sp_count, tokens, LANES), bf16),
            vmem((tokens, 3 * WIN_ROWS // 2 * GRID_W), f32),
        ],
        flops=5 * 10**9,
    )
    attended = lax.all_to_all(attended, ("sp", "tp"), 0, 0, tiled=True)
    own_rows = lax.dynamic_slice_in_dim(latent, tp_index * out_rows, out_rows, 0)
    return call(
        functools.partial(output_kernel, sp_count=sp_count, tp_count=tp_count),
        shape((out_rows, model_width), bf16),
        (
            indices,
            in_vmem(attended),
            own_rows,
            gating,
            gain_post.reshape(1, -1),
            *gates,
            w_out,
            near,
            far,
            relayed,
        ),
        scratch=[vmem((tp_count, out_rows, cols), bf16), vmem((tp_count, cols, model_width), bf16), dma((tp_count,))],
        scalars=1,
        raw=tp_count,
        flops=10**9,
    )


def solution(mesh):
    in_specs = (
        P("sp", None),
        P("sp", None),
        P(),
        P(),
        P(),
        P(),
        P("sp", "tp"),
        P("sp", "tp"),
        P("sp", "tp"),
        P(None, "tp"),
        P(None, "tp"),
        P(None, "tp"),
        P(None, "tp"),
        P("tp", None, None),
        P("tp", None),
    )
    out_specs = P(("sp", "tp"), None)
    sp_count, tp_count = mesh.shape["sp"], mesh.shape["tp"]

    def shards(*arrays):
        heads = arrays[13].shape[0]
        head_width = arrays[6].shape[1] // heads
        grid_rows = arrays[0].shape[0] // GRID_W
        one_head_each = (
            heads == sp_count
            and sp_count >= 3
            and tp_count == 4
            and head_width == HALF
            and GRID_W == HALF
            and 2 * grid_rows == WIN_ROWS
        )
        return (shards_by_heads if one_head_each else shards_by_rows)(*arrays)

    return jax.shard_map(shards, mesh=mesh, in_specs=in_specs, out_specs=out_specs, check_vma=False)
```

```python
import functools

import jax
import jax.numpy as jnp
import numpy as np
from jax import lax
from jax.experimental import pallas as pl
from jax.experimental.pallas import tpu as pltpu
from jax.sharding import PartitionSpec as P


GRID_W = 64
WIN_ROWS = 8
WIN_COLS = 16
LANES = 128
HALF = LANES // 2
HIDDEN_SCORE = -1e30

EPSILON = 1e-06


def extended_2(cells, sides, width):
    for axis, dim in sides:
        count = lax.axis_size(axis)
        ends = count - 1
        head = lax.slice_in_dim(cells, 0, width, axis=dim)
        tail = lax.slice_in_dim(cells, cells.shape[dim] - width, cells.shape[dim], axis=dim)
        cells = jnp.concatenate(
            [
                lax.ppermute(tail, axis, [(i, (i + 1) % count) for i in range(ends)]),
                cells,
                lax.ppermute(head, axis, [((i + 1) % count, i) for i in range(ends)]),
            ],
            axis=dim,
        )
    return cells


def normalize(row_block, gain_row):
    values = row_block.astype(jnp.float32)
    return (
        values * lax.rsqrt(jnp.mean(values * values, axis=-1, keepdims=True) + EPSILON) * gain_row
    )


def modulate(row_block, gain_row, shift_row, scale_row):
    return (normalize(row_block, gain_row) * (1.0 + scale_row) + shift_row).astype(jnp.bfloat16)


def product(left, right):
    return jnp.dot(left, right, preferred_element_type=jnp.float32)


def shards_by_rows(
    latent,
    context,
    condition,
    context_condition,
    gain_pre,
    gain_post,
    w_shift,
    w_scale,
    w_gate,
    w_query,
    w_key,
    w_value,
    w_silu,
    offset_bias,
    w_out,
):
    sp_index = lax.axis_index("sp")
    tp_index = lax.axis_index("tp")
    in_rows, local_cols = w_shift.shape
    tokens, _ = latent.shape
    active = jax.nn.silu(jnp.stack([condition, context_condition]).astype(jnp.float32)).astype(
        jnp.bfloat16
    )
    own_active = lax.dynamic_slice_in_dim(active, sp_index * in_rows, in_rows, 1)
    stacked = jnp.stack([w_shift, w_scale, w_gate])
    partial_value = jnp.einsum(
        "ai,mij->maj", own_active, stacked, preferred_element_type=jnp.float32
    )
    summed = lax.psum(partial_value, "sp")
    modulation = lax.all_gather(summed, "tp", axis=2, tiled=True)
    shifts, scales, gating = (modulation[0], modulation[1], modulation[2])
    normed = modulate(context, gain_pre, shifts[1], scales[1])
    context_kv = lax.all_gather(
        jnp.concatenate([product(normed, w_key), product(normed, w_value)], axis=1).astype(
            jnp.bfloat16
        ),
        "sp",
        axis=0,
        tiled=True,
    )
    hidden = modulate(latent, gain_pre, shifts[0], scales[0])
    queries = product(hidden, w_query).astype(jnp.bfloat16)
    keys_latent = product(hidden, w_key).astype(jnp.bfloat16)
    values_latent = product(hidden, w_value).astype(jnp.bfloat16)
    silu_gate = product(hidden, w_silu).astype(jnp.bfloat16)
    head_count = offset_bias.shape[0]
    head_width = local_cols // head_count
    grid_rows = tokens // GRID_W
    kv_grid = jnp.concatenate([keys_latent, values_latent], axis=1).reshape(
        grid_rows, GRID_W, 2 * local_cols
    )
    extended = extended_2(kv_grid, (("sp", 0),), WIN_ROWS // 2)
    blocks = GRID_W // WIN_COLS
    key_span = 2 * WIN_COLS
    block_start = np.clip(np.arange(blocks) * WIN_COLS - WIN_COLS // 2, 0, GRID_W - key_span)
    query_col = np.arange(blocks)[:, None] * WIN_COLS + np.arange(WIN_COLS)[None, :]
    key_col = block_start[:, None] + np.arange(key_span)[None, :]
    window_start = np.clip(query_col - WIN_COLS // 2, 0, GRID_W - WIN_COLS)
    inside_cols = (key_col[:, None, :] >= window_start[:, :, None]) & (
        key_col[:, None, :] < window_start[:, :, None] + WIN_COLS
    )
    inside_window = np.broadcast_to(
        inside_cols[:, :, None, :], (blocks, WIN_COLS, WIN_ROWS, key_span)
    ).reshape(blocks, WIN_COLS, WIN_ROWS * key_span)[None, :, None, :, :]
    col_offset = np.clip(
        key_col[:, None, :] - query_col[:, :, None] + WIN_COLS - 1, 0, 2 * WIN_COLS - 2
    )
    col_table = (col_offset[..., None] == np.arange(2 * WIN_COLS - 1)).astype(np.float32)
    total_rows = grid_rows * lax.axis_size("sp")
    local_rows = jnp.arange(grid_rows, dtype=jnp.int32)
    global_row = sp_index * grid_rows + local_rows
    row_start = jnp.clip(global_row - WIN_ROWS // 2, 0, total_rows - WIN_ROWS)
    band_first = row_start - sp_index * grid_rows + WIN_ROWS // 2
    row_offset = (
        row_start[:, None]
        + jnp.arange(WIN_ROWS, dtype=jnp.int32)[None, :]
        - global_row[:, None]
        + WIN_ROWS
        - 1
    )
    row_table = (row_offset[..., None] == jnp.arange(2 * WIN_ROWS - 1, dtype=jnp.int32)).astype(
        jnp.float32
    )
    position = (
        band_first[:, None, None, None] + jnp.arange(WIN_ROWS, dtype=jnp.int32)[None, None, :, None]
    ) * GRID_W + jnp.asarray(key_col, jnp.int32)[None, :, None, :]
    flat_rows = extended.reshape(-1, 2 * local_cols)
    window_kv = jnp.take(flat_rows, position.reshape(-1), axis=0).reshape(
        grid_rows, blocks, WIN_ROWS * key_span, 2 * local_cols
    )
    window_keys = window_kv[..., :local_cols].reshape(
        grid_rows, blocks, WIN_ROWS * key_span, head_count, head_width
    )
    window_values = window_kv[..., local_cols:].reshape(
        grid_rows, blocks, WIN_ROWS * key_span, head_count, head_width
    )
    context_keys = context_kv[:, :local_cols].reshape(-1, head_count, head_width)
    context_values = context_kv[:, local_cols:].reshape(-1, head_count, head_width)
    query_blocks = queries.reshape(grid_rows, blocks, WIN_COLS, head_count, head_width)
    score_scale = head_width ** (-0.5)
    by_column = jnp.einsum(
        "hae,bqwe->hbqwa", offset_bias, jnp.asarray(col_table), precision=lax.Precision.HIGHEST
    )
    offset_terms = jnp.einsum(
        "rva,hbqwa->rbhqvw", row_table, by_column, precision=lax.Precision.HIGHEST
    ).reshape(grid_rows, blocks, head_count, WIN_COLS, WIN_ROWS * key_span)
    window_scores = (
        jnp.einsum(
            "rbqhd,rbkhd->rbhqk", query_blocks, window_keys, preferred_element_type=jnp.float32
        )
        * score_scale
    )
    window_scores = jnp.where(inside_window, window_scores + offset_terms, -jnp.inf)
    context_scores = (
        jnp.einsum(
            "rbqhd,khd->rbhqk", query_blocks, context_keys, preferred_element_type=jnp.float32
        )
        * score_scale
    )
    maximum = jnp.maximum(jnp.max(window_scores, axis=-1), jnp.max(context_scores, axis=-1))[
        ..., None
    ]
    window_exp = jnp.exp(window_scores - maximum)
    context_exp = jnp.exp(context_scores - maximum)
    denominator = jnp.sum(window_exp, axis=-1, keepdims=True) + jnp.sum(
        context_exp, axis=-1, keepdims=True
    )
    window_weights = (window_exp / denominator).astype(jnp.bfloat16)
    context_weights = (context_exp / denominator).astype(jnp.bfloat16)
    attended = jnp.einsum(
        "rbhqk,rbkhd->rbqhd", window_weights, window_values, preferred_element_type=jnp.float32
    )
    attended = attended + jnp.einsum(
        "rbhqk,khd->rbqhd", context_weights, context_values, preferred_element_type=jnp.float32
    )
    attended = attended.reshape(tokens, local_cols)
    gated_heads = (jax.nn.silu(silu_gate.astype(jnp.float32)) * attended).astype(jnp.bfloat16)
    out_rows = tokens // lax.axis_size("tp")
    branch = lax.psum_scatter(
        product(gated_heads, w_out).astype(jnp.bfloat16), "tp", scatter_dimension=0, tiled=True
    )
    own_rows = lax.dynamic_slice_in_dim(latent, tp_index * out_rows, out_rows, 0)
    updated = own_rows.astype(jnp.float32) + gating[0] * normalize(branch, gain_post)
    return updated.astype(jnp.bfloat16)


def low_half(shape):
    return lax.broadcasted_iota(jnp.int32, shape, len(shape) - 1) < HALF


def swap_halves(block):
    return pltpu.roll(block, HALF, len(block.shape) - 1)


def head_pair(first, second):
    low = low_half(first.shape)
    return (
        jnp.where(low, first, swap_halves(second)),
        jnp.where(low, swap_halves(first), second),
    )


def partial_kernel(
    condition_ref, context_ref, shift_ref, scale_ref, gate_ref, out_ref, active_ref
):
    rows = shift_ref.shape[0] // LANES
    for kind, source in enumerate((condition_ref, context_ref)):
        values = source[...].astype(jnp.float32)
        active_ref[kind] = values / (1.0 + jnp.exp(-values))
    own = pl.ds(lax.axis_index("sp") * rows, rows)
    vectors = [active_ref[kind, own, :].astype(jnp.bfloat16) for kind in range(2)]
    width = shift_ref.shape[1] // LANES
    row = 0
    for weight_ref, kinds in ((shift_ref, 2), (scale_ref, 2), (gate_ref, 1)):
        both = sum(
            jnp.dot(
                jnp.concatenate([vectors[kind][part : part + 1] for kind in range(2)], axis=0),
                weight_ref[part * LANES : (part + 1) * LANES, :],
                preferred_element_type=jnp.float32,
            )
            for part in range(rows)
        )
        for kind in range(kinds):
            for lane in range(width):
                block = both[kind : kind + 1, lane * LANES : (lane + 1) * LANES].astype(out_ref.dtype)
                out_ref[:, row : row + 1, :] = jnp.broadcast_to(block[None], (out_ref.shape[0], 1, LANES))
                row += 1


def norms(values):
    mean = jnp.sum(values * values, axis=-1, keepdims=True) * (1.0 / values.shape[-1])
    return lax.rsqrt(mean + EPSILON)


def norm_kernel(
    latent_ref, before_ref, after_ref, context_hbm, out_ref, before_out, after_out, half_ref, semaphore
):
    count = half_ref.shape[0]
    first = pl.multiple_of(lax.axis_index("tp") % 2 * count, count)
    copy = pltpu.make_async_copy(context_hbm.at[pl.ds(first, count)], half_ref, semaphore)
    copy.start()
    before_out[...] = jnp.broadcast_to(before_ref[...], before_out.shape)
    after_out[...] = jnp.broadcast_to(after_ref[...], after_out.shape)
    step = 32

    def body(index, carry):
        rows = pl.ds(pl.multiple_of(index * step, step), step)
        norm = norms(latent_ref[rows, :].astype(jnp.float32))
        out_ref[rows, :] = jnp.broadcast_to(norm, (step, LANES))
        return carry

    lax.fori_loop(0, latent_ref.shape[0] // step, body, 0)
    copy.wait()


def modulate_rows(source, target, first, count, vectors_ref, gain_ref, kind, norm_ref=None):
    factor = gain_ref[:1, :] * (1.0 + vectors_ref[2 + kind : 3 + kind, :])
    shift = vectors_ref[kind : kind + 1, :]
    step = 32

    def body(index, carry):
        start = pl.multiple_of(index * step, step)
        values = source[pl.ds(start, step), :].astype(jnp.float32)
        norm = norms(values) if norm_ref is None else norm_ref[pl.ds(start, step), :][:, :1]
        target[pl.ds(pl.multiple_of(first + start, step), step), :] = (
            values * norm * factor + shift
        ).astype(jnp.bfloat16)
        return carry

    lax.fori_loop(0, count // step, body, 0)


def start_all(pairs, semaphores):
    copies = [
        pltpu.make_async_copy(source, target, semaphores.at[index])
        for index, (source, target) in enumerate(pairs)
    ]
    for copy in copies:
        copy.start()
    return copies


def project_kernel(
    terms_ref, latent_hbm, norm_hbm, gain_hbm, key_hbm, value_hbm, query_hbm,
    send_hbm, hidden_hbm, vectors_hbm,
    latent_ref, norm_ref, gain_ref, key_ref, value_ref, query_ref,
    send_ref, hidden_ref, vectors_ref, loads, stores,
    *, sp_count, tp_count
):
    copies = start_all(
        (
            (norm_hbm, norm_ref),
            (gain_hbm, gain_ref),
            (latent_hbm, latent_ref),
            (key_hbm, key_ref),
            (value_hbm, value_ref),
            (query_hbm, query_ref),
        ),
        loads,
    )
    saves = []

    def save(source, target):
        saves.append(pltpu.make_async_copy(source, target, stores.at[len(saves)]))
        saves[-1].start()

    cols = key_ref.shape[1]
    width = cols // LANES
    for part in range(tp_count):
        total = terms_ref[part].astype(jnp.float32)
        for other in range(1, sp_count):
            total = total + terms_ref[other * tp_count + part].astype(jnp.float32)
        for index in range(5):
            for lane in range(width):
                first = part * cols + lane * LANES
                row = index * width + lane
                vectors_ref[index : index + 1, first : first + LANES] = total[row : row + 1]
    vectors_ref[5:, :] = jnp.zeros((vectors_ref.shape[0] - 5, vectors_ref.shape[1]), jnp.float32)
    save(vectors_ref, vectors_hbm)
    tokens = latent_ref.shape[0]
    half = tokens // 2
    for copy in copies[:3]:
        copy.wait()
    modulate_rows(latent_ref, hidden_ref, 0, tokens, vectors_ref, gain_ref, 0, norm_ref)
    save(hidden_ref, hidden_hbm)
    copies[3].wait()
    keys = jnp.dot(hidden_ref[...], key_ref[...], preferred_element_type=jnp.float32)
    copies[4].wait()
    values = jnp.dot(hidden_ref[...], value_ref[...], preferred_element_type=jnp.float32)
    for pair in range(width):
        lanes = slice(pair * LANES, (pair + 1) * LANES)
        for head, kv in enumerate(head_pair(keys[:, lanes], values[:, lanes])):
            send_ref[2 * pair + head, :tokens, :] = kv.astype(jnp.bfloat16)
    save(send_ref.at[:, pl.ds(0, tokens)], send_hbm.at[:, pl.ds(0, tokens)])
    copies[5].wait()
    queries = jnp.dot(hidden_ref[...], query_ref[...], preferred_element_type=jnp.float32)
    for pair in range(width):
        lanes = slice(pair * LANES, (pair + 1) * LANES)
        block = queries[:, lanes].astype(jnp.bfloat16).astype(jnp.float32) * HALF**-0.5
        for head, packed in enumerate(head_pair(block[:half], block[half:])):
            send_ref[2 * pair + head, tokens:, :] = packed.astype(jnp.bfloat16)
    save(send_ref.at[:, pl.ds(tokens, half)], send_hbm.at[:, pl.ds(tokens, half)])
    for copy in saves:
        copy.wait()


def context_kernel(*refs, sp_count, sources):
    heads = sp_count // 2
    source_refs, (vectors_hbm, gain_hbm, key_hbm, value_hbm) = refs[:sources], refs[sources : sources + 4]
    outs, refs = refs[sources + 4 : sources + 4 + heads], refs[sources + 4 + heads :]
    (vectors_ref, gain_ref, key_ref, value_ref, hidden_ref, send_ref, loads, stores) = refs
    own = lax.axis_index("sp")
    width = key_ref.shape[1]
    cols = pl.ds(pl.multiple_of(own // heads * width, width), width)
    copies = start_all(
        (
            (vectors_hbm, vectors_ref),
            (gain_hbm, gain_ref),
            (key_hbm.at[:, cols], key_ref),
            (value_hbm.at[:, cols], value_ref),
        ),
        loads,
    )
    for copy in copies[:2]:
        copy.wait()
    first = 0
    for source in source_refs:
        modulate_rows(source, hidden_ref, first, source.shape[0], vectors_ref, gain_ref, 1)
        first += source.shape[0]
    copies[2].wait()
    keys = jnp.dot(hidden_ref[...], key_ref[...], preferred_element_type=jnp.float32)
    copies[3].wait()
    values = jnp.dot(hidden_ref[...], value_ref[...], preferred_element_type=jnp.float32)
    for pair in range(heads // 2):
        lanes = slice(pair * LANES, (pair + 1) * LANES)
        for head, kv in enumerate(head_pair(keys[:, lanes], values[:, lanes])):
            send_ref[2 * pair + head] = kv.astype(jnp.bfloat16)
    for copy in start_all(
        [(send_ref.at[own % heads ^ offset], out) for offset, out in enumerate(outs)], stores
    ):
        copy.wait()


def gate_kernel(hidden_ref, weight_ref, *out_refs):
    *out_refs, rows_ref = out_refs
    rows_ref[...] = jnp.dot(hidden_ref[...], weight_ref[...], preferred_element_type=jnp.float32)
    for offset, out_ref in enumerate(out_refs):
        count = out_ref.shape[0]
        first = pl.multiple_of((lax.axis_index("tp") ^ offset) * count, count)
        out_ref[...] = rows_ref[pl.ds(first, count), :].astype(jnp.bfloat16)


def bias_kernel(table_ref, pairs_ref, rows_ref):
    rows_ref[...] = jnp.zeros_like(rows_ref)
    own = pl.ds(lax.axis_index("sp"), 1)
    for index in range(table_ref.shape[0]):
        rows_ref[index : index + 1, : table_ref.shape[2]] = table_ref[index, own, :]
    column = lax.broadcasted_iota(jnp.int32, (GRID_W, LANES), 0)
    key_column = lax.broadcasted_iota(jnp.int32, (GRID_W, LANES), 1) % GRID_W
    first_column = jnp.clip(column - WIN_COLS // 2, 0, GRID_W - WIN_COLS)
    inside = (key_column >= first_column) & (key_column < first_column + WIN_COLS)
    count = pairs_ref.shape[0]
    first = pltpu.roll(rows_ref[...], LANES - WIN_COLS + 1, 1)
    second = pltpu.roll(rows_ref[...], HALF - WIN_COLS + 1, 1)
    for index in range(count):
        row = first[index : index + 1] + second[index + 1 : index + 2]
        toeplitz = pltpu.roll(jnp.broadcast_to(row, (GRID_W, LANES)), 0, 1, stride=1, stride_axis=0)
        pairs_ref[index] = jnp.where(inside, toeplitz, HIDDEN_SCORE)


def fill_bias(bias_ref, pairs_ref, block, blocks):
    tokens, band = bias_ref.shape
    grid_rows, band_rows = tokens // GRID_W, band // GRID_W
    total_rows = blocks * grid_rows
    hidden = jnp.full((GRID_W, LANES), HIDDEN_SCORE, jnp.float32)
    low = low_half(hidden.shape)
    last = pairs_ref.shape[0] - 1
    band_first = min(max(block * grid_rows - WIN_ROWS // 2, 0), total_rows - band_rows)
    for query in range(grid_rows):
        query_row = block * grid_rows + query
        window_first = min(max(query_row - WIN_ROWS // 2, 0), total_rows - WIN_ROWS)
        for pair in range(band_rows // 2):
            key_row = band_first + 2 * pair
            valid = [window_first <= key_row + side < window_first + WIN_ROWS for side in range(2)]
            offset = key_row - query_row + WIN_ROWS - 1
            if not any(valid):
                tile = hidden
            elif 0 <= offset <= last:
                tile = pairs_ref[offset]
            else:
                tile = swap_halves(pairs_ref[last if offset > last else 0])
            if any(valid) and not all(valid):
                tile = jnp.where(low if valid[0] else ~low, tile, hidden)
            bias_ref[
                query * GRID_W : (query + 1) * GRID_W, pair * LANES : (pair + 1) * LANES
            ] = tile


def with_ones(kv):
    return jnp.where(low_half(kv.shape), jnp.ones_like(kv), kv)


CONTRACT_LANES = (((1,), (1,)), ((), ()))


def attend_kernel(received_ref, *refs):
    *sources, pairs_hbm, out_hbm = refs[:-8]
    pairs_ref, out_ref, ones_ref, context_ref, context_ones_ref, query_ref, bias_ref, semaphores = refs[-8:]
    blocks = received_ref.shape[0]
    tokens = query_ref.shape[1]
    rows = context_ref.shape[0] // len(sources)
    loads = start_all([(pairs_hbm, pairs_ref)], semaphores)
    for index, source in enumerate(sources):
        kv = source[...]
        context_ref[index * rows : (index + 1) * rows, :] = kv
        context_ones_ref[index * rows : (index + 1) * rows, :] = with_ones(kv)
    parts = out_ref.shape[0] // blocks
    chunk = tokens // parts
    half = tokens // 2
    for block in range(blocks):
        ones_ref[block * tokens : (block + 1) * tokens, :] = with_ones(received_ref[block, :tokens, :])
        packed = received_ref[block, tokens:, :].astype(jnp.float32)
        low = low_half(packed.shape)
        query_ref[block, :half, :] = jnp.where(low, packed, 0.0).astype(jnp.bfloat16)
        query_ref[block, half:, :] = jnp.where(low, swap_halves(packed), 0.0).astype(jnp.bfloat16)
    for load in loads:
        load.wait()
    low = low_half((chunk // 2, LANES))
    saves = []
    for block in range(blocks):
        if block in (0, 1, blocks - 1):
            fill_bias(bias_ref, pairs_ref, block, blocks)
        band = min(max(block - 1, 0), blocks - 3)
        queries = query_ref[block]
        context = lax.dot_general(
            queries, context_ref[...], CONTRACT_LANES, preferred_element_type=jnp.float32
        )
        window = jnp.concatenate(
            [
                lax.dot_general(
                    queries,
                    received_ref[band + part, :tokens, :],
                    CONTRACT_LANES,
                    preferred_element_type=jnp.float32,
                )
                for part in range(3)
            ],
            axis=1,
        ) + bias_ref[...]
        maximum = jnp.maximum(
            jnp.max(window, axis=-1, keepdims=True), jnp.max(context, axis=-1, keepdims=True)
        )
        sums = jnp.dot(
            jnp.exp(context - maximum).astype(jnp.bfloat16),
            context_ones_ref[...],
            preferred_element_type=jnp.float32,
        ) + jnp.dot(
            jnp.exp(window - maximum).astype(jnp.bfloat16),
            ones_ref[band * tokens : (band + 3) * tokens, :],
            preferred_element_type=jnp.float32,
        )
        attended = sums / swap_halves(sums)
        for part in range(parts):
            rows = attended[part * chunk : (part + 1) * chunk]
            out_ref[block * parts + part] = jnp.where(
                low, swap_halves(rows[: chunk // 2]), rows[chunk // 2 :]
            ).astype(jnp.bfloat16)
        own = pl.ds(block * parts, parts)
        saves.append(pltpu.make_async_copy(out_ref.at[own], out_hbm.at[own], semaphores.at[block]))
        saves[-1].start()
    for save in saves:
        save.wait()


def output_kernel(attended_ref, *refs, sp_count, tp_count):
    small = 3
    gate_refs, refs = refs[:tp_count], refs[tp_count:]
    sources, weights, refs = refs[:small], refs[small : small + tp_count], refs[small + tp_count :]
    out_ref, gated_ref, weight_ref, *targets, semaphores = refs
    pieces = (semaphores.shape[0] - small) // tp_count
    depth = weight_ref.shape[1] // pieces
    pairs = list(zip(sources, targets)) + [
        (source.at[rows], weight_ref.at[index, rows])
        for index, source in enumerate(weights)
        for rows in (pl.ds(piece * depth, depth) for piece in range(pieces))
    ]
    copies = [
        pltpu.make_async_copy(source, target, semaphores.at[index])
        for index, (source, target) in enumerate(pairs)
    ]
    for copy in copies:
        copy.start()
    latent_ref, vectors_ref, gain_ref = targets
    half = attended_ref.shape[1]
    for offset in range(tp_count):
        group = lax.axis_index("tp") ^ offset
        for pair in range(sp_count // 2):
            first = attended_ref[2 * pair * tp_count + group].astype(jnp.float32)
            second = attended_ref[(2 * pair + 1) * tp_count + group].astype(jnp.float32)
            lanes = slice(pair * LANES, (pair + 1) * LANES)
            for side, block in enumerate(head_pair(first, second)):
                gate = gate_refs[offset][side * half : (side + 1) * half, lanes].astype(jnp.float32)
                gated_ref[offset, side * half : (side + 1) * half, lanes] = (
                    gate / (1.0 + jnp.exp(-gate)) * block
                ).astype(jnp.bfloat16)
    total = None
    for index, copy in enumerate(copies[small:]):
        offset, piece = divmod(index, pieces)
        rows = slice(piece * depth, (piece + 1) * depth)
        copy.wait()
        term = jnp.dot(
            gated_ref[offset, :, rows], weight_ref[offset, rows, :], preferred_element_type=jnp.float32
        )
        total = term if total is None else total + term
    for copy in copies[:small]:
        copy.wait()
    branch = total.astype(jnp.bfloat16).astype(jnp.float32)
    mean = jnp.sum(branch * branch, axis=-1, keepdims=True) * (1.0 / branch.shape[-1])
    out_ref[...] = (
        latent_ref[...].astype(jnp.float32)
        + vectors_ref[4:5, :] * (branch * lax.rsqrt(mean + EPSILON)) * gain_ref[:1, :]
    ).astype(jnp.bfloat16)


def in_vmem(array):
    return pltpu.with_memory_space_constraint(array, pltpu.VMEM)


def call(kernel, out_shape, operands, scratch=(), raw=0, raw_outs=(), flops=0, mib=58):
    vmem, hbm = pl.BlockSpec(), pl.BlockSpec(memory_space=pl.ANY)
    single = not isinstance(out_shape, tuple)
    out_specs = [
        hbm if index in raw_outs else vmem for index in range(1 if single else len(out_shape))
    ]
    return pl.pallas_call(
        kernel,
        in_specs=[vmem] * (len(operands) - raw) + [hbm] * raw,
        out_specs=out_specs[0] if single else out_specs,
        out_shape=out_shape,
        scratch_shapes=scratch,
        cost_estimate=pl.CostEstimate(flops=flops, transcendentals=0, bytes_accessed=0),
        compiler_params=pltpu.CompilerParams(vmem_limit_bytes=mib * 2**20),
    )(*operands)


def shards_by_heads(
    latent,
    context,
    condition,
    context_condition,
    gain_pre,
    gain_post,
    w_shift,
    w_scale,
    w_gate,
    w_query,
    w_key,
    w_value,
    w_silu,
    offset_bias,
    w_out,
):
    tp_index = lax.axis_index("tp")
    sp_count, tp_count = lax.axis_size("sp"), lax.axis_size("tp")
    cols = w_shift.shape[1]
    tokens, model_width = latent.shape
    context_tokens = context.shape[0]
    rows = tokens + tokens // 2
    width = cols // LANES
    f32, bf16 = jnp.float32, jnp.bfloat16
    vmem = pltpu.VMEM

    shape = jax.ShapeDtypeStruct
    across = [(index, index ^ (tp_count // 2)) for index in range(tp_count)]
    beside = [(index, index ^ 1) for index in range(tp_count)]
    dma = pltpu.SemaphoreType.DMA

    terms = call(
        partial_kernel,
        shape((sp_count * tp_count, 5 * width, LANES), bf16),
        (
            condition.reshape(-1, LANES),
            context_condition.reshape(-1, LANES),
            w_shift,
            w_scale,
            w_gate,
        ),
        scratch=[vmem((2, model_width // LANES, LANES), f32)],
    )
    terms = lax.all_to_all(terms, ("sp", "tp"), 0, 0, tiled=True)
    far = lax.ppermute(w_out, "tp", across)
    near = lax.ppermute(w_out, "tp", beside)
    norm, gain, gain_after, context_half = call(
        norm_kernel,
        (
            shape((tokens, LANES), f32),
            shape((8, model_width), f32),
            shape((8, model_width), f32),
            shape((context_tokens // 2, model_width), bf16),
        ),
        (latent, gain_pre.reshape(1, -1), gain_post.reshape(1, -1), context),
        raw=1,
        scratch=[dma],
        flops=3 * 10**9,
    )
    opposite = [(index, index ^ (sp_count // 2)) for index in range(sp_count)]
    far_context = lax.ppermute(context_half, "sp", opposite)
    offsets = offset_bias.shape[1]
    pairs = call(
        bias_kernel,
        shape((offsets - 1, GRID_W, LANES), f32),
        (jnp.transpose(offset_bias, (1, 0, 2)),),
        scratch=[vmem((16, LANES), f32)],
        flops=3 * 10**9,
    )
    send, hidden, vectors = call(
        functools.partial(project_kernel, sp_count=sp_count, tp_count=tp_count),
        (
            shape((sp_count, rows, LANES), bf16),
            shape((tokens, model_width), bf16),
            shape((8, model_width), f32),
        ),
        (in_vmem(terms), latent, norm, gain, w_key, w_value, w_query),
        raw=6,
        raw_outs=(0, 1, 2),
        scratch=[
            vmem(latent.shape, bf16),
            vmem(norm.shape, f32),
            vmem((8, model_width), f32),
            vmem(w_key.shape, bf16),
            vmem(w_value.shape, bf16),
            vmem(w_query.shape, bf16),
            vmem((sp_count, rows, LANES), bf16),
            vmem(latent.shape, bf16),
            vmem((8, model_width), f32),
            dma((6,)),
            dma((4,)),
        ],
        flops=10**9,
    )
    received = lax.all_to_all(send, "sp", 0, 0, tiled=True)
    group = sp_count // 2

    def context_heads(*sources):
        count = sum(source.shape[0] for source in sources)
        return call(
            functools.partial(context_kernel, sp_count=sp_count, sources=len(sources)),
            (shape((count, LANES), bf16),) * group,
            (*sources, vectors, gain, w_key, w_value),
            raw=4,
            raw_outs=tuple(range(group)),
            scratch=[
                vmem((8, model_width), f32),
                vmem((8, model_width), f32),
                vmem((model_width, cols // 2), bf16),
                vmem((model_width, cols // 2), bf16),
                vmem((count, model_width), bf16),
                vmem((group, count, LANES), bf16),
                dma((4,)),
                dma((group,)),
            ],
            flops=10**9,
        )

    def context_exchange(parts):
        return [parts[0]] + [
            lax.ppermute(
                parts[offset], "sp", [(index, index ^ offset) for index in range(sp_count)]
            )
            for offset in range(1, group)
        ]

    context_kv = context_exchange(context_heads(context))
    near_context = lax.ppermute(far_context, "tp", beside)
    context_kv += context_exchange(context_heads(in_vmem(far_context), in_vmem(near_context)))
    out_rows = tokens // tp_count
    gates = call(
        gate_kernel,
        (shape((out_rows, cols), bf16),) * tp_count,
        (hidden, w_silu),
        scratch=[vmem((tokens, cols), f32)],
        flops=10**9,
    )
    gates = [gates[0]] + [
        lax.ppermute(gates[offset], "tp", [(index, index ^ offset) for index in range(tp_count)])
        for offset in range(1, tp_count)
    ]
    relayed = lax.ppermute(far, "tp", beside)
    attended = call(
        attend_kernel,
        shape((sp_count * tp_count, out_rows // 2, LANES), bf16),
        (in_vmem(received), *map(in_vmem, context_kv), pairs),
        raw=1,
        raw_outs=(0,),
        scratch=[
            vmem(pairs.shape, f32),
            vmem((sp_count * tp_count, out_rows // 2, LANES), bf16),
            vmem((sp_count * tokens, LANES), bf16),
            vmem((sp_count * context_tokens, LANES), bf16),
            vmem((sp_count * context_tokens, LANES), bf16),
            vmem((sp_count, tokens, LANES), bf16),
            vmem((tokens, 3 * tokens), f32),
            dma((sp_count,)),
        ],
        flops=5 * 10**9,
    )
    attended = lax.all_to_all(attended, ("sp", "tp"), 0, 0, tiled=True)
    own_rows = lax.dynamic_slice_in_dim(latent, tp_index * out_rows, out_rows, 0)
    return call(
        functools.partial(output_kernel, sp_count=sp_count, tp_count=tp_count),
        shape((out_rows, model_width), bf16),
        (
            in_vmem(attended),
            *map(in_vmem, gates),
            own_rows,
            vectors,
            gain_after,
            w_out,
            near,
            far,
            relayed,
        ),
        scratch=[
            vmem((tp_count, out_rows, cols), bf16),
            vmem((tp_count, cols, model_width), bf16),
            vmem((out_rows, model_width), bf16),
            vmem((8, model_width), f32),
            vmem((8, model_width), f32),
            dma((2 * tp_count + 3,)),
        ],
        raw=tp_count + 3,
        flops=10**9,
    )


def solution(mesh):
    in_specs = (
        P("sp", None),
        P("sp", None),
        P(),
        P(),
        P(),
        P(),
        P("sp", "tp"),
        P("sp", "tp"),
        P("sp", "tp"),
        P(None, "tp"),
        P(None, "tp"),
        P(None, "tp"),
        P(None, "tp"),
        P("tp", None, None),
        P("tp", None),
    )
    out_specs = P(("sp", "tp"), None)
    sp_count, tp_count = mesh.shape["sp"], mesh.shape["tp"]

    def shards(*arrays):
        heads = arrays[13].shape[0]
        head_width = arrays[6].shape[1] // heads
        grid_rows = arrays[0].shape[0] // GRID_W
        one_head_each = (
            heads == sp_count
            and tp_count == 4
            and sp_count == 8
            and head_width == HALF
            and GRID_W == HALF
            and 2 * grid_rows == WIN_ROWS
        )
        return (shards_by_heads if one_head_each else shards_by_rows)(*arrays)

    return jax.shard_map(shards, mesh=mesh, in_specs=in_specs, out_specs=out_specs, check_vma=False)
```

```python
import functools

import jax
import jax.numpy as jnp
import numpy as np
from jax import lax
from jax.experimental import pallas as pl
from jax.experimental.pallas import tpu as pltpu
from jax.sharding import PartitionSpec as P


GRID_W = 64
WIN_ROWS = 8
WIN_COLS = 16
LANES = 128
HALF = LANES // 2
HIDDEN_SCORE = -1e30

EPSILON = 1e-06


def extended_2(cells, sides, width):
    for axis, dim in sides:
        count = lax.axis_size(axis)
        ends = count - 1
        head = lax.slice_in_dim(cells, 0, width, axis=dim)
        tail = lax.slice_in_dim(cells, cells.shape[dim] - width, cells.shape[dim], axis=dim)
        cells = jnp.concatenate(
            [
                lax.ppermute(tail, axis, [(i, (i + 1) % count) for i in range(ends)]),
                cells,
                lax.ppermute(head, axis, [((i + 1) % count, i) for i in range(ends)]),
            ],
            axis=dim,
        )
    return cells


def normalize(row_block, gain_row):
    values = row_block.astype(jnp.float32)
    return (
        values * lax.rsqrt(jnp.mean(values * values, axis=-1, keepdims=True) + EPSILON) * gain_row
    )


def modulate(row_block, gain_row, shift_row, scale_row):
    return (normalize(row_block, gain_row) * (1.0 + scale_row) + shift_row).astype(jnp.bfloat16)


def product(left, right):
    return jnp.dot(left, right, preferred_element_type=jnp.float32)


def shards_by_rows(
    latent,
    context,
    condition,
    context_condition,
    gain_pre,
    gain_post,
    w_shift,
    w_scale,
    w_gate,
    w_query,
    w_key,
    w_value,
    w_silu,
    offset_bias,
    w_out,
):
    sp_index = lax.axis_index("sp")
    tp_index = lax.axis_index("tp")
    in_rows, local_cols = w_shift.shape
    tokens, _ = latent.shape
    active = jax.nn.silu(jnp.stack([condition, context_condition]).astype(jnp.float32)).astype(
        jnp.bfloat16
    )
    own_active = lax.dynamic_slice_in_dim(active, sp_index * in_rows, in_rows, 1)
    stacked = jnp.stack([w_shift, w_scale, w_gate])
    partial_value = jnp.einsum(
        "ai,mij->maj", own_active, stacked, preferred_element_type=jnp.float32
    )
    summed = lax.psum(partial_value, "sp")
    modulation = lax.all_gather(summed, "tp", axis=2, tiled=True)
    shifts, scales, gating = (modulation[0], modulation[1], modulation[2])
    normed = modulate(context, gain_pre, shifts[1], scales[1])
    context_kv = lax.all_gather(
        jnp.concatenate([product(normed, w_key), product(normed, w_value)], axis=1).astype(
            jnp.bfloat16
        ),
        "sp",
        axis=0,
        tiled=True,
    )
    hidden = modulate(latent, gain_pre, shifts[0], scales[0])
    queries = product(hidden, w_query).astype(jnp.bfloat16)
    keys_latent = product(hidden, w_key).astype(jnp.bfloat16)
    values_latent = product(hidden, w_value).astype(jnp.bfloat16)
    silu_gate = product(hidden, w_silu).astype(jnp.bfloat16)
    head_count = offset_bias.shape[0]
    head_width = local_cols // head_count
    grid_rows = tokens // GRID_W
    kv_grid = jnp.concatenate([keys_latent, values_latent], axis=1).reshape(
        grid_rows, GRID_W, 2 * local_cols
    )
    extended = extended_2(kv_grid, (("sp", 0),), WIN_ROWS // 2)
    blocks = GRID_W // WIN_COLS
    key_span = 2 * WIN_COLS
    block_start = np.clip(np.arange(blocks) * WIN_COLS - WIN_COLS // 2, 0, GRID_W - key_span)
    query_col = np.arange(blocks)[:, None] * WIN_COLS + np.arange(WIN_COLS)[None, :]
    key_col = block_start[:, None] + np.arange(key_span)[None, :]
    window_start = np.clip(query_col - WIN_COLS // 2, 0, GRID_W - WIN_COLS)
    inside_cols = (key_col[:, None, :] >= window_start[:, :, None]) & (
        key_col[:, None, :] < window_start[:, :, None] + WIN_COLS
    )
    inside_window = np.broadcast_to(
        inside_cols[:, :, None, :], (blocks, WIN_COLS, WIN_ROWS, key_span)
    ).reshape(blocks, WIN_COLS, WIN_ROWS * key_span)[None, :, None, :, :]
    col_offset = np.clip(
        key_col[:, None, :] - query_col[:, :, None] + WIN_COLS - 1, 0, 2 * WIN_COLS - 2
    )
    col_table = (col_offset[..., None] == np.arange(2 * WIN_COLS - 1)).astype(np.float32)
    total_rows = grid_rows * lax.axis_size("sp")
    local_rows = jnp.arange(grid_rows, dtype=jnp.int32)
    global_row = sp_index * grid_rows + local_rows
    row_start = jnp.clip(global_row - WIN_ROWS // 2, 0, total_rows - WIN_ROWS)
    band_first = row_start - sp_index * grid_rows + WIN_ROWS // 2
    row_offset = (
        row_start[:, None]
        + jnp.arange(WIN_ROWS, dtype=jnp.int32)[None, :]
        - global_row[:, None]
        + WIN_ROWS
        - 1
    )
    row_table = (row_offset[..., None] == jnp.arange(2 * WIN_ROWS - 1, dtype=jnp.int32)).astype(
        jnp.float32
    )
    position = (
        band_first[:, None, None, None] + jnp.arange(WIN_ROWS, dtype=jnp.int32)[None, None, :, None]
    ) * GRID_W + jnp.asarray(key_col, jnp.int32)[None, :, None, :]
    flat_rows = extended.reshape(-1, 2 * local_cols)
    window_kv = jnp.take(flat_rows, position.reshape(-1), axis=0).reshape(
        grid_rows, blocks, WIN_ROWS * key_span, 2 * local_cols
    )
    window_keys = window_kv[..., :local_cols].reshape(
        grid_rows, blocks, WIN_ROWS * key_span, head_count, head_width
    )
    window_values = window_kv[..., local_cols:].reshape(
        grid_rows, blocks, WIN_ROWS * key_span, head_count, head_width
    )
    context_keys = context_kv[:, :local_cols].reshape(-1, head_count, head_width)
    context_values = context_kv[:, local_cols:].reshape(-1, head_count, head_width)
    query_blocks = queries.reshape(grid_rows, blocks, WIN_COLS, head_count, head_width)
    score_scale = head_width ** (-0.5)
    by_column = jnp.einsum(
        "hae,bqwe->hbqwa", offset_bias, jnp.asarray(col_table), precision=lax.Precision.HIGHEST
    )
    offset_terms = jnp.einsum(
        "rva,hbqwa->rbhqvw", row_table, by_column, precision=lax.Precision.HIGHEST
    ).reshape(grid_rows, blocks, head_count, WIN_COLS, WIN_ROWS * key_span)
    window_scores = (
        jnp.einsum(
            "rbqhd,rbkhd->rbhqk", query_blocks, window_keys, preferred_element_type=jnp.float32
        )
        * score_scale
    )
    window_scores = jnp.where(inside_window, window_scores + offset_terms, -jnp.inf)
    context_scores = (
        jnp.einsum(
            "rbqhd,khd->rbhqk", query_blocks, context_keys, preferred_element_type=jnp.float32
        )
        * score_scale
    )
    maximum = jnp.maximum(jnp.max(window_scores, axis=-1), jnp.max(context_scores, axis=-1))[
        ..., None
    ]
    window_exp = jnp.exp(window_scores - maximum)
    context_exp = jnp.exp(context_scores - maximum)
    denominator = jnp.sum(window_exp, axis=-1, keepdims=True) + jnp.sum(
        context_exp, axis=-1, keepdims=True
    )
    window_weights = (window_exp / denominator).astype(jnp.bfloat16)
    context_weights = (context_exp / denominator).astype(jnp.bfloat16)
    attended = jnp.einsum(
        "rbhqk,rbkhd->rbqhd", window_weights, window_values, preferred_element_type=jnp.float32
    )
    attended = attended + jnp.einsum(
        "rbhqk,khd->rbqhd", context_weights, context_values, preferred_element_type=jnp.float32
    )
    attended = attended.reshape(tokens, local_cols)
    gated_heads = (jax.nn.silu(silu_gate.astype(jnp.float32)) * attended).astype(jnp.bfloat16)
    out_rows = tokens // lax.axis_size("tp")
    branch = lax.psum_scatter(
        product(gated_heads, w_out).astype(jnp.bfloat16), "tp", scatter_dimension=0, tiled=True
    )
    own_rows = lax.dynamic_slice_in_dim(latent, tp_index * out_rows, out_rows, 0)
    updated = own_rows.astype(jnp.float32) + gating[0] * normalize(branch, gain_post)
    return updated.astype(jnp.bfloat16)


def low_half(shape):
    return lax.broadcasted_iota(jnp.int32, shape, len(shape) - 1) < HALF


def swap_halves(block):
    return pltpu.roll(block, HALF, len(block.shape) - 1)


def head_pair(first, second):
    low = low_half(first.shape)
    return (
        jnp.where(low, first, swap_halves(second)),
        jnp.where(low, swap_halves(first), second),
    )


def partial_kernel(
    condition_ref, context_ref, shift_ref, scale_ref, gate_ref, out_ref, active_ref
):
    rows = shift_ref.shape[0] // LANES
    for kind, source in enumerate((condition_ref, context_ref)):
        values = source[...].astype(jnp.float32)
        active_ref[kind] = values / (1.0 + jnp.exp(-values))
    own = pl.ds(lax.axis_index("sp") * rows, rows)
    vectors = [active_ref[kind, own, :].astype(jnp.bfloat16) for kind in range(2)]
    width = shift_ref.shape[1] // LANES
    row = 0
    for weight_ref, kinds in ((shift_ref, 2), (scale_ref, 2), (gate_ref, 1)):
        both = sum(
            jnp.dot(
                jnp.concatenate([vectors[kind][part : part + 1] for kind in range(2)], axis=0),
                weight_ref[part * LANES : (part + 1) * LANES, :],
                preferred_element_type=jnp.float32,
            )
            for part in range(rows)
        )
        for kind in range(kinds):
            for lane in range(width):
                block = both[kind : kind + 1, lane * LANES : (lane + 1) * LANES].astype(out_ref.dtype)
                out_ref[:, row : row + 1, :] = jnp.broadcast_to(block[None], (out_ref.shape[0], 1, LANES))
                row += 1


def norms(values):
    mean = jnp.sum(values * values, axis=-1, keepdims=True) * (1.0 / values.shape[-1])
    return lax.rsqrt(mean + EPSILON)


def norm_kernel(
    latent_ref, before_ref, after_ref, context_hbm, out_ref, before_out, after_out, half_ref, semaphore
):
    count = half_ref.shape[0]
    first = pl.multiple_of(lax.axis_index("tp") % 2 * count, count)
    copy = pltpu.make_async_copy(context_hbm.at[pl.ds(first, count)], half_ref, semaphore)
    copy.start()
    before_out[...] = jnp.broadcast_to(before_ref[...], before_out.shape)
    after_out[...] = jnp.broadcast_to(after_ref[...], after_out.shape)
    step = 32

    def body(index, carry):
        rows = pl.ds(pl.multiple_of(index * step, step), step)
        norm = norms(latent_ref[rows, :].astype(jnp.float32))
        out_ref[rows, :] = jnp.broadcast_to(norm, (step, LANES))
        return carry

    lax.fori_loop(0, latent_ref.shape[0] // step, body, 0)
    copy.wait()


def modulate_rows(source, target, first, count, vectors_ref, gain_ref, kind, norm_ref=None):
    factor = gain_ref[:1, :] * (1.0 + vectors_ref[2 + kind : 3 + kind, :])
    shift = vectors_ref[kind : kind + 1, :]
    step = 32

    def body(index, carry):
        start = pl.multiple_of(index * step, step)
        values = source[pl.ds(start, step), :].astype(jnp.float32)
        norm = norms(values) if norm_ref is None else norm_ref[pl.ds(start, step), :][:, :1]
        target[pl.ds(pl.multiple_of(first + start, step), step), :] = (
            values * norm * factor + shift
        ).astype(jnp.bfloat16)
        return carry

    lax.fori_loop(0, count // step, body, 0)


def start_all(pairs, semaphores):
    copies = [
        pltpu.make_async_copy(source, target, semaphores.at[index])
        for index, (source, target) in enumerate(pairs)
    ]
    for copy in copies:
        copy.start()
    return copies


def project_kernel(
    terms_ref, latent_hbm, norm_hbm, gain_hbm, key_hbm, value_hbm, query_hbm,
    send_hbm, hidden_hbm, vectors_hbm,
    latent_ref, norm_ref, gain_ref, key_ref, value_ref, query_ref,
    send_ref, hidden_ref, vectors_ref, loads, stores,
    *, sp_count, tp_count
):
    half_cols = query_ref.shape[1] // 2
    copies = start_all(
        (
            (norm_hbm, norm_ref),
            (gain_hbm, gain_ref),
            (latent_hbm, latent_ref),
            (key_hbm, key_ref),
            (value_hbm, value_ref),
            (query_hbm.at[:, pl.ds(0, half_cols)], query_ref.at[:, pl.ds(0, half_cols)]),
            (query_hbm.at[:, pl.ds(half_cols, half_cols)], query_ref.at[:, pl.ds(half_cols, half_cols)]),
        ),
        loads,
    )
    saves = []

    def save(source, target):
        saves.append(pltpu.make_async_copy(source, target, stores.at[len(saves)]))
        saves[-1].start()

    cols = key_ref.shape[1]
    width = cols // LANES
    for part in range(tp_count):
        total = terms_ref[part].astype(jnp.float32)
        for other in range(1, sp_count):
            total = total + terms_ref[other * tp_count + part].astype(jnp.float32)
        for index in range(5):
            for lane in range(width):
                first = part * cols + lane * LANES
                row = index * width + lane
                vectors_ref[index : index + 1, first : first + LANES] = total[row : row + 1]
    vectors_ref[5:, :] = jnp.zeros((vectors_ref.shape[0] - 5, vectors_ref.shape[1]), jnp.float32)
    save(vectors_ref, vectors_hbm)
    tokens = latent_ref.shape[0]
    half = tokens // 2
    for copy in copies[:3]:
        copy.wait()
    modulate_rows(latent_ref, hidden_ref, 0, tokens, vectors_ref, gain_ref, 0, norm_ref)
    save(hidden_ref, hidden_hbm)
    copies[3].wait()
    keys = jnp.dot(hidden_ref[...], key_ref[...], preferred_element_type=jnp.float32)
    copies[4].wait()
    values = jnp.dot(hidden_ref[...], value_ref[...], preferred_element_type=jnp.float32)
    for pair in range(width):
        lanes = slice(pair * LANES, (pair + 1) * LANES)
        for head, kv in enumerate(head_pair(keys[:, lanes], values[:, lanes])):
            send_ref[2 * pair + head, :tokens, :] = kv.astype(jnp.bfloat16)
    save(send_ref.at[:, pl.ds(0, tokens)], send_hbm.at[:, pl.ds(0, tokens)])
    for pair in range(width):
        if pair % (width // 2) == 0:
            part = pair // (width // 2)
            copies[5 + part].wait()
            queries = jnp.dot(
                hidden_ref[...],
                query_ref[:, part * half_cols : (part + 1) * half_cols],
                preferred_element_type=jnp.float32,
            )
        first = pair * LANES - part * half_cols
        block = queries[:, first : first + LANES].astype(jnp.bfloat16).astype(jnp.float32) * HALF**-0.5
        for head, packed in enumerate(head_pair(block[:half], block[half:])):
            send_ref[2 * pair + head, tokens:, :] = packed.astype(jnp.bfloat16)
    save(send_ref.at[:, pl.ds(tokens, half)], send_hbm.at[:, pl.ds(tokens, half)])
    for copy in saves:
        copy.wait()


def context_kernel(*refs, sp_count, sources):
    heads = sp_count // 2
    source_refs, (vectors_hbm, gain_hbm, key_hbm, value_hbm) = refs[:sources], refs[sources : sources + 4]
    outs, refs = refs[sources + 4 : sources + 4 + heads], refs[sources + 4 + heads :]
    (vectors_ref, gain_ref, key_ref, value_ref, hidden_ref, send_ref, loads, stores) = refs
    own = lax.axis_index("sp")
    width = key_ref.shape[1]
    cols = pl.ds(pl.multiple_of(own // heads * width, width), width)
    copies = start_all(
        (
            (vectors_hbm, vectors_ref),
            (gain_hbm, gain_ref),
            (key_hbm.at[:, cols], key_ref),
            (value_hbm.at[:, cols], value_ref),
        ),
        loads,
    )
    for copy in copies[:2]:
        copy.wait()
    first = 0
    for source in source_refs:
        modulate_rows(source, hidden_ref, first, source.shape[0], vectors_ref, gain_ref, 1)
        first += source.shape[0]
    copies[2].wait()
    keys = jnp.dot(hidden_ref[...], key_ref[...], preferred_element_type=jnp.float32)
    copies[3].wait()
    values = jnp.dot(hidden_ref[...], value_ref[...], preferred_element_type=jnp.float32)
    for pair in range(heads // 2):
        lanes = slice(pair * LANES, (pair + 1) * LANES)
        for head, kv in enumerate(head_pair(keys[:, lanes], values[:, lanes])):
            send_ref[2 * pair + head] = kv.astype(jnp.bfloat16)
    for copy in start_all(
        [(send_ref.at[own % heads ^ offset], out) for offset, out in enumerate(outs)], stores
    ):
        copy.wait()


def gate_kernel(hidden_ref, weight_ref, *out_refs):
    *out_refs, rows_ref = out_refs
    rows_ref[...] = jnp.dot(hidden_ref[...], weight_ref[...], preferred_element_type=jnp.float32)
    for offset, out_ref in enumerate(out_refs):
        count = out_ref.shape[0]
        first = pl.multiple_of((lax.axis_index("tp") ^ offset) * count, count)
        out_ref[...] = rows_ref[pl.ds(first, count), :].astype(jnp.bfloat16)


def bias_kernel(table_ref, pairs_ref, rows_ref):
    rows_ref[...] = jnp.zeros_like(rows_ref)
    own = pl.ds(lax.axis_index("sp"), 1)
    for index in range(table_ref.shape[0]):
        rows_ref[index : index + 1, : table_ref.shape[2]] = table_ref[index, own, :]
    column = lax.broadcasted_iota(jnp.int32, (GRID_W, LANES), 0)
    key_column = lax.broadcasted_iota(jnp.int32, (GRID_W, LANES), 1) % GRID_W
    first_column = jnp.clip(column - WIN_COLS // 2, 0, GRID_W - WIN_COLS)
    inside = (key_column >= first_column) & (key_column < first_column + WIN_COLS)
    count = pairs_ref.shape[0]
    first = pltpu.roll(rows_ref[...], LANES - WIN_COLS + 1, 1)
    second = pltpu.roll(rows_ref[...], HALF - WIN_COLS + 1, 1)
    for index in range(count):
        row = first[index : index + 1] + second[index + 1 : index + 2]
        toeplitz = pltpu.roll(jnp.broadcast_to(row, (GRID_W, LANES)), 0, 1, stride=1, stride_axis=0)
        pairs_ref[index] = jnp.where(inside, toeplitz, HIDDEN_SCORE)


def fill_bias(bias_ref, pairs_ref, block, blocks):
    tokens, band = bias_ref.shape
    grid_rows, band_rows = tokens // GRID_W, band // GRID_W
    total_rows = blocks * grid_rows
    hidden = jnp.full((GRID_W, LANES), HIDDEN_SCORE, jnp.float32)
    low = low_half(hidden.shape)
    last = pairs_ref.shape[0] - 1
    band_first = min(max(block * grid_rows - WIN_ROWS // 2, 0), total_rows - band_rows)
    for query in range(grid_rows):
        query_row = block * grid_rows + query
        window_first = min(max(query_row - WIN_ROWS // 2, 0), total_rows - WIN_ROWS)
        for pair in range(band_rows // 2):
            key_row = band_first + 2 * pair
            valid = [window_first <= key_row + side < window_first + WIN_ROWS for side in range(2)]
            offset = key_row - query_row + WIN_ROWS - 1
            if not any(valid):
                tile = hidden
            elif 0 <= offset <= last:
                tile = pairs_ref[offset]
            else:
                tile = swap_halves(pairs_ref[last if offset > last else 0])
            if any(valid) and not all(valid):
                tile = jnp.where(low if valid[0] else ~low, tile, hidden)
            bias_ref[
                query * GRID_W : (query + 1) * GRID_W, pair * LANES : (pair + 1) * LANES
            ] = tile


def with_ones(kv):
    return jnp.where(low_half(kv.shape), jnp.ones_like(kv), kv)


CONTRACT_LANES = (((1,), (1,)), ((), ()))


def attend_kernel(received_ref, *refs):
    *sources, pairs_hbm, out_hbm = refs[:-8]
    pairs_ref, out_ref, ones_ref, context_ref, context_ones_ref, query_ref, bias_ref, semaphores = refs[-8:]
    blocks = received_ref.shape[0]
    tokens = query_ref.shape[1]
    rows = context_ref.shape[0] // len(sources)
    loads = start_all([(pairs_hbm, pairs_ref)], semaphores)
    for index, source in enumerate(sources):
        kv = source[...]
        context_ref[index * rows : (index + 1) * rows, :] = kv
        context_ones_ref[index * rows : (index + 1) * rows, :] = with_ones(kv)
    parts = out_ref.shape[0] // blocks
    chunk = tokens // parts
    half = tokens // 2
    for block in range(blocks):
        ones_ref[block * tokens : (block + 1) * tokens, :] = with_ones(received_ref[block, :tokens, :])
        packed = received_ref[block, tokens:, :].astype(jnp.float32)
        low = low_half(packed.shape)
        query_ref[block, :half, :] = jnp.where(low, packed, 0.0).astype(jnp.bfloat16)
        query_ref[block, half:, :] = jnp.where(low, swap_halves(packed), 0.0).astype(jnp.bfloat16)
    for load in loads:
        load.wait()
    low = low_half((chunk // 2, LANES))
    saves = []
    for block in range(blocks):
        if block in (0, 1, blocks - 1):
            fill_bias(bias_ref, pairs_ref, block, blocks)
        band = min(max(block - 1, 0), blocks - 3)
        queries = query_ref[block]
        context = lax.dot_general(
            queries, context_ref[...], CONTRACT_LANES, preferred_element_type=jnp.float32
        )
        window = jnp.concatenate(
            [
                lax.dot_general(
                    queries,
                    received_ref[band + part, :tokens, :],
                    CONTRACT_LANES,
                    preferred_element_type=jnp.float32,
                )
                for part in range(3)
            ],
            axis=1,
        ) + bias_ref[...]
        maximum = jnp.maximum(
            jnp.max(window, axis=-1, keepdims=True), jnp.max(context, axis=-1, keepdims=True)
        )
        sums = jnp.dot(
            jnp.exp(context - maximum).astype(jnp.bfloat16),
            context_ones_ref[...],
            preferred_element_type=jnp.float32,
        ) + jnp.dot(
            jnp.exp(window - maximum).astype(jnp.bfloat16),
            ones_ref[band * tokens : (band + 3) * tokens, :],
            preferred_element_type=jnp.float32,
        )
        attended = sums / swap_halves(sums)
        for part in range(parts):
            rows = attended[part * chunk : (part + 1) * chunk]
            out_ref[block * parts + part] = jnp.where(
                low, swap_halves(rows[: chunk // 2]), rows[chunk // 2 :]
            ).astype(jnp.bfloat16)
        own = pl.ds(block * parts, parts)
        saves.append(pltpu.make_async_copy(out_ref.at[own], out_hbm.at[own], semaphores.at[block]))
        saves[-1].start()
    for save in saves:
        save.wait()


def output_kernel(attended_ref, own_weight_ref, *refs, sp_count, tp_count):
    small = 3
    gate_refs, refs = refs[:tp_count], refs[tp_count:]
    sources, refs = refs[:small], refs[small:]
    weights, refs = refs[: tp_count - 1], refs[tp_count - 1 :]
    out_ref, gated_ref, weight_ref, *targets, semaphores = refs
    count = targets[0].shape[0]
    own = pl.ds(pl.multiple_of(lax.axis_index("tp") * count, count), count)
    sources = (sources[0].at[own], *sources[1:])
    pieces = (semaphores.shape[0] - small) // (tp_count - 1)
    depth = weight_ref.shape[1] // pieces
    pairs = list(zip(sources, targets)) + [
        (source.at[rows], weight_ref.at[index, rows])
        for index, source in enumerate(weights)
        for rows in (pl.ds(piece * depth, depth) for piece in range(pieces))
    ]
    copies = [
        pltpu.make_async_copy(source, target, semaphores.at[index])
        for index, (source, target) in enumerate(pairs)
    ]
    for copy in copies:
        copy.start()
    latent_ref, vectors_ref, gain_ref = targets
    half = attended_ref.shape[1]
    for offset in range(tp_count):
        group = lax.axis_index("tp") ^ offset
        for pair in range(sp_count // 2):
            first = attended_ref[2 * pair * tp_count + group].astype(jnp.float32)
            second = attended_ref[(2 * pair + 1) * tp_count + group].astype(jnp.float32)
            lanes = slice(pair * LANES, (pair + 1) * LANES)
            for side, block in enumerate(head_pair(first, second)):
                gate = gate_refs[offset][side * half : (side + 1) * half, lanes].astype(jnp.float32)
                gated_ref[offset, side * half : (side + 1) * half, lanes] = (
                    gate / (1.0 + jnp.exp(-gate)) * block
                ).astype(jnp.bfloat16)
    total = jnp.dot(gated_ref[0], own_weight_ref[...], preferred_element_type=jnp.float32)
    for index, copy in enumerate(copies[small:]):
        offset, piece = divmod(index, pieces)
        rows = slice(piece * depth, (piece + 1) * depth)
        copy.wait()
        total = total + jnp.dot(
            gated_ref[1 + offset, :, rows],
            weight_ref[offset, rows, :],
            preferred_element_type=jnp.float32,
        )
    for copy in copies[:small]:
        copy.wait()
    branch = total.astype(jnp.bfloat16).astype(jnp.float32)
    mean = jnp.sum(branch * branch, axis=-1, keepdims=True) * (1.0 / branch.shape[-1])
    out_ref[...] = (
        latent_ref[...].astype(jnp.float32)
        + vectors_ref[4:5, :] * (branch * lax.rsqrt(mean + EPSILON)) * gain_ref[:1, :]
    ).astype(jnp.bfloat16)


def in_vmem(array):
    return pltpu.with_memory_space_constraint(array, pltpu.VMEM)


def call(kernel, out_shape, operands, scratch=(), raw=0, raw_outs=(), flops=0, mib=58):
    vmem, hbm = pl.BlockSpec(), pl.BlockSpec(memory_space=pl.ANY)
    single = not isinstance(out_shape, tuple)
    out_specs = [
        hbm if index in raw_outs else vmem for index in range(1 if single else len(out_shape))
    ]
    return pl.pallas_call(
        kernel,
        in_specs=[vmem] * (len(operands) - raw) + [hbm] * raw,
        out_specs=out_specs[0] if single else out_specs,
        out_shape=out_shape,
        scratch_shapes=scratch,
        cost_estimate=pl.CostEstimate(flops=flops, transcendentals=0, bytes_accessed=0),
        compiler_params=pltpu.CompilerParams(vmem_limit_bytes=mib * 2**20),
    )(*operands)


def shards_by_heads(
    latent,
    context,
    condition,
    context_condition,
    gain_pre,
    gain_post,
    w_shift,
    w_scale,
    w_gate,
    w_query,
    w_key,
    w_value,
    w_silu,
    offset_bias,
    w_out,
):
    sp_count, tp_count = lax.axis_size("sp"), lax.axis_size("tp")
    cols = w_shift.shape[1]
    tokens, model_width = latent.shape
    context_tokens = context.shape[0]
    rows = tokens + tokens // 2
    width = cols // LANES
    f32, bf16 = jnp.float32, jnp.bfloat16
    vmem = pltpu.VMEM

    shape = jax.ShapeDtypeStruct
    across = [(index, index ^ (tp_count // 2)) for index in range(tp_count)]
    beside = [(index, index ^ 1) for index in range(tp_count)]
    dma = pltpu.SemaphoreType.DMA

    terms = call(
        partial_kernel,
        shape((sp_count * tp_count, 5 * width, LANES), bf16),
        (
            condition.reshape(-1, LANES),
            context_condition.reshape(-1, LANES),
            w_shift,
            w_scale,
            w_gate,
        ),
        scratch=[vmem((2, model_width // LANES, LANES), f32)],
    )
    terms = lax.all_to_all(terms, ("sp", "tp"), 0, 0, tiled=True)
    far = lax.ppermute(w_out, "tp", across)
    near = lax.ppermute(w_out, "tp", beside)
    norm, gain, gain_after, context_half = call(
        norm_kernel,
        (
            shape((tokens, LANES), f32),
            shape((8, model_width), f32),
            shape((8, model_width), f32),
            shape((context_tokens // 2, model_width), bf16),
        ),
        (latent, gain_pre.reshape(1, -1), gain_post.reshape(1, -1), context),
        raw=1,
        scratch=[dma],
        flops=3 * 10**9,
    )
    opposite = [(index, index ^ (sp_count // 2)) for index in range(sp_count)]
    far_context = lax.ppermute(context_half, "sp", opposite)
    offsets = offset_bias.shape[1]
    pairs = call(
        bias_kernel,
        shape((offsets - 1, GRID_W, LANES), f32),
        (jnp.transpose(offset_bias, (1, 0, 2)),),
        scratch=[vmem((16, LANES), f32)],
        flops=3 * 10**9,
    )
    send, hidden, vectors = call(
        functools.partial(project_kernel, sp_count=sp_count, tp_count=tp_count),
        (
            shape((sp_count, rows, LANES), bf16),
            shape((tokens, model_width), bf16),
            shape((8, model_width), f32),
        ),
        (in_vmem(terms), latent, norm, gain, w_key, w_value, w_query),
        raw=6,
        raw_outs=(0, 1, 2),
        scratch=[
            vmem(latent.shape, bf16),
            vmem(norm.shape, f32),
            vmem((8, model_width), f32),
            vmem(w_key.shape, bf16),
            vmem(w_value.shape, bf16),
            vmem(w_query.shape, bf16),
            vmem((sp_count, rows, LANES), bf16),
            vmem(latent.shape, bf16),
            vmem((8, model_width), f32),
            dma((7,)),
            dma((4,)),
        ],
        flops=10**9,
    )
    received = lax.all_to_all(send, "sp", 0, 0, tiled=True)
    group = sp_count // 2

    def context_heads(*sources):
        count = sum(source.shape[0] for source in sources)
        return call(
            functools.partial(context_kernel, sp_count=sp_count, sources=len(sources)),
            (shape((count, LANES), bf16),) * group,
            (*sources, vectors, gain, w_key, w_value),
            raw=4,
            raw_outs=tuple(range(group)),
            scratch=[
                vmem((8, model_width), f32),
                vmem((8, model_width), f32),
                vmem((model_width, cols // 2), bf16),
                vmem((model_width, cols // 2), bf16),
                vmem((count, model_width), bf16),
                vmem((group, count, LANES), bf16),
                dma((4,)),
                dma((group,)),
            ],
            flops=10**9,
        )

    def context_exchange(parts):
        return [parts[0]] + [
            lax.ppermute(
                parts[offset], "sp", [(index, index ^ offset) for index in range(sp_count)]
            )
            for offset in range(1, group)
        ]

    context_kv = context_exchange(context_heads(context))
    near_context = lax.ppermute(far_context, "tp", beside)
    context_kv += context_exchange(context_heads(in_vmem(far_context), in_vmem(near_context)))
    out_rows = tokens // tp_count
    gates = call(
        gate_kernel,
        (shape((out_rows, cols), bf16),) * tp_count,
        (hidden, w_silu),
        scratch=[vmem((tokens, cols), f32)],
        flops=10**9,
    )
    gates = [gates[0]] + [
        lax.ppermute(gates[offset], "tp", [(index, index ^ offset) for index in range(tp_count)])
        for offset in range(1, tp_count)
    ]
    relayed = lax.ppermute(far, "tp", beside)
    attended = call(
        attend_kernel,
        shape((sp_count * tp_count, out_rows // 2, LANES), bf16),
        (in_vmem(received), *map(in_vmem, context_kv), pairs),
        raw=1,
        raw_outs=(0,),
        scratch=[
            vmem(pairs.shape, f32),
            vmem((sp_count * tp_count, out_rows // 2, LANES), bf16),
            vmem((sp_count * tokens, LANES), bf16),
            vmem((sp_count * context_tokens, LANES), bf16),
            vmem((sp_count * context_tokens, LANES), bf16),
            vmem((sp_count, tokens, LANES), bf16),
            vmem((tokens, 3 * tokens), f32),
            dma((sp_count,)),
        ],
        flops=5 * 10**9,
    )
    attended = lax.all_to_all(attended, ("sp", "tp"), 0, 0, tiled=True)
    return call(
        functools.partial(output_kernel, sp_count=sp_count, tp_count=tp_count),
        shape((out_rows, model_width), bf16),
        (
            in_vmem(attended),
            in_vmem(w_out),
            *map(in_vmem, gates),
            latent,
            vectors,
            gain_after,
            near,
            far,
            relayed,
        ),
        scratch=[
            vmem((tp_count, out_rows, cols), bf16),
            vmem((tp_count - 1, cols, model_width), bf16),
            vmem((out_rows, model_width), bf16),
            vmem((8, model_width), f32),
            vmem((8, model_width), f32),
            dma((2 * tp_count + 1,)),
        ],
        raw=tp_count + 2,
        flops=10**9,
    )


def solution(mesh):
    in_specs = (
        P("sp", None),
        P("sp", None),
        P(),
        P(),
        P(),
        P(),
        P("sp", "tp"),
        P("sp", "tp"),
        P("sp", "tp"),
        P(None, "tp"),
        P(None, "tp"),
        P(None, "tp"),
        P(None, "tp"),
        P("tp", None, None),
        P("tp", None),
    )
    out_specs = P(("sp", "tp"), None)
    sp_count, tp_count = mesh.shape["sp"], mesh.shape["tp"]

    def shards(*arrays):
        heads = arrays[13].shape[0]
        head_width = arrays[6].shape[1] // heads
        grid_rows = arrays[0].shape[0] // GRID_W
        one_head_each = (
            heads == sp_count
            and tp_count == 4
            and sp_count == 8
            and head_width == HALF
            and GRID_W == HALF
            and 2 * grid_rows == WIN_ROWS
        )
        return (shards_by_heads if one_head_each else shards_by_rows)(*arrays)

    return jax.shard_map(shards, mesh=mesh, in_specs=in_specs, out_specs=out_specs, check_vma=False)
```

```python
import functools

import jax
import jax.numpy as jnp
import numpy as np
from jax import lax
from jax.experimental import pallas as pl
from jax.experimental.pallas import tpu as pltpu
from jax.sharding import PartitionSpec as P


GRID_W = 64
WIN_ROWS = 8
WIN_COLS = 16
LANES = 128
HALF = LANES // 2
HIDDEN_SCORE = -1e30

EPSILON = 1e-06


def extended_2(cells, sides, width):
    for axis, dim in sides:
        count = lax.axis_size(axis)
        ends = count - 1
        head = lax.slice_in_dim(cells, 0, width, axis=dim)
        tail = lax.slice_in_dim(cells, cells.shape[dim] - width, cells.shape[dim], axis=dim)
        cells = jnp.concatenate(
            [
                lax.ppermute(tail, axis, [(i, (i + 1) % count) for i in range(ends)]),
                cells,
                lax.ppermute(head, axis, [((i + 1) % count, i) for i in range(ends)]),
            ],
            axis=dim,
        )
    return cells


def normalize(row_block, gain_row):
    values = row_block.astype(jnp.float32)
    return (
        values * lax.rsqrt(jnp.mean(values * values, axis=-1, keepdims=True) + EPSILON) * gain_row
    )


def modulate(row_block, gain_row, shift_row, scale_row):
    return (normalize(row_block, gain_row) * (1.0 + scale_row) + shift_row).astype(jnp.bfloat16)


def product(left, right):
    return jnp.dot(left, right, preferred_element_type=jnp.float32)


def shards_by_rows(
    latent,
    context,
    condition,
    context_condition,
    gain_pre,
    gain_post,
    w_shift,
    w_scale,
    w_gate,
    w_query,
    w_key,
    w_value,
    w_silu,
    offset_bias,
    w_out,
):
    sp_index = lax.axis_index("sp")
    tp_index = lax.axis_index("tp")
    in_rows, local_cols = w_shift.shape
    tokens, _ = latent.shape
    active = jax.nn.silu(jnp.stack([condition, context_condition]).astype(jnp.float32)).astype(
        jnp.bfloat16
    )
    own_active = lax.dynamic_slice_in_dim(active, sp_index * in_rows, in_rows, 1)
    stacked = jnp.stack([w_shift, w_scale, w_gate])
    partial_value = jnp.einsum(
        "ai,mij->maj", own_active, stacked, preferred_element_type=jnp.float32
    )
    summed = lax.psum(partial_value, "sp")
    modulation = lax.all_gather(summed, "tp", axis=2, tiled=True)
    shifts, scales, gating = (modulation[0], modulation[1], modulation[2])
    normed = modulate(context, gain_pre, shifts[1], scales[1])
    context_kv = lax.all_gather(
        jnp.concatenate([product(normed, w_key), product(normed, w_value)], axis=1).astype(
            jnp.bfloat16
        ),
        "sp",
        axis=0,
        tiled=True,
    )
    hidden = modulate(latent, gain_pre, shifts[0], scales[0])
    queries = product(hidden, w_query).astype(jnp.bfloat16)
    keys_latent = product(hidden, w_key).astype(jnp.bfloat16)
    values_latent = product(hidden, w_value).astype(jnp.bfloat16)
    silu_gate = product(hidden, w_silu).astype(jnp.bfloat16)
    head_count = offset_bias.shape[0]
    head_width = local_cols // head_count
    grid_rows = tokens // GRID_W
    kv_grid = jnp.concatenate([keys_latent, values_latent], axis=1).reshape(
        grid_rows, GRID_W, 2 * local_cols
    )
    extended = extended_2(kv_grid, (("sp", 0),), WIN_ROWS // 2)
    blocks = GRID_W // WIN_COLS
    key_span = 2 * WIN_COLS
    block_start = np.clip(np.arange(blocks) * WIN_COLS - WIN_COLS // 2, 0, GRID_W - key_span)
    query_col = np.arange(blocks)[:, None] * WIN_COLS + np.arange(WIN_COLS)[None, :]
    key_col = block_start[:, None] + np.arange(key_span)[None, :]
    window_start = np.clip(query_col - WIN_COLS // 2, 0, GRID_W - WIN_COLS)
    inside_cols = (key_col[:, None, :] >= window_start[:, :, None]) & (
        key_col[:, None, :] < window_start[:, :, None] + WIN_COLS
    )
    inside_window = np.broadcast_to(
        inside_cols[:, :, None, :], (blocks, WIN_COLS, WIN_ROWS, key_span)
    ).reshape(blocks, WIN_COLS, WIN_ROWS * key_span)[None, :, None, :, :]
    col_offset = np.clip(
        key_col[:, None, :] - query_col[:, :, None] + WIN_COLS - 1, 0, 2 * WIN_COLS - 2
    )
    col_table = (col_offset[..., None] == np.arange(2 * WIN_COLS - 1)).astype(np.float32)
    total_rows = grid_rows * lax.axis_size("sp")
    local_rows = jnp.arange(grid_rows, dtype=jnp.int32)
    global_row = sp_index * grid_rows + local_rows
    row_start = jnp.clip(global_row - WIN_ROWS // 2, 0, total_rows - WIN_ROWS)
    band_first = row_start - sp_index * grid_rows + WIN_ROWS // 2
    row_offset = (
        row_start[:, None]
        + jnp.arange(WIN_ROWS, dtype=jnp.int32)[None, :]
        - global_row[:, None]
        + WIN_ROWS
        - 1
    )
    row_table = (row_offset[..., None] == jnp.arange(2 * WIN_ROWS - 1, dtype=jnp.int32)).astype(
        jnp.float32
    )
    position = (
        band_first[:, None, None, None] + jnp.arange(WIN_ROWS, dtype=jnp.int32)[None, None, :, None]
    ) * GRID_W + jnp.asarray(key_col, jnp.int32)[None, :, None, :]
    flat_rows = extended.reshape(-1, 2 * local_cols)
    window_kv = jnp.take(flat_rows, position.reshape(-1), axis=0).reshape(
        grid_rows, blocks, WIN_ROWS * key_span, 2 * local_cols
    )
    window_keys = window_kv[..., :local_cols].reshape(
        grid_rows, blocks, WIN_ROWS * key_span, head_count, head_width
    )
    window_values = window_kv[..., local_cols:].reshape(
        grid_rows, blocks, WIN_ROWS * key_span, head_count, head_width
    )
    context_keys = context_kv[:, :local_cols].reshape(-1, head_count, head_width)
    context_values = context_kv[:, local_cols:].reshape(-1, head_count, head_width)
    query_blocks = queries.reshape(grid_rows, blocks, WIN_COLS, head_count, head_width)
    score_scale = head_width ** (-0.5)
    by_column = jnp.einsum(
        "hae,bqwe->hbqwa", offset_bias, jnp.asarray(col_table), precision=lax.Precision.HIGHEST
    )
    offset_terms = jnp.einsum(
        "rva,hbqwa->rbhqvw", row_table, by_column, precision=lax.Precision.HIGHEST
    ).reshape(grid_rows, blocks, head_count, WIN_COLS, WIN_ROWS * key_span)
    window_scores = (
        jnp.einsum(
            "rbqhd,rbkhd->rbhqk", query_blocks, window_keys, preferred_element_type=jnp.float32
        )
        * score_scale
    )
    window_scores = jnp.where(inside_window, window_scores + offset_terms, -jnp.inf)
    context_scores = (
        jnp.einsum(
            "rbqhd,khd->rbhqk", query_blocks, context_keys, preferred_element_type=jnp.float32
        )
        * score_scale
    )
    maximum = jnp.maximum(jnp.max(window_scores, axis=-1), jnp.max(context_scores, axis=-1))[
        ..., None
    ]
    window_exp = jnp.exp(window_scores - maximum)
    context_exp = jnp.exp(context_scores - maximum)
    denominator = jnp.sum(window_exp, axis=-1, keepdims=True) + jnp.sum(
        context_exp, axis=-1, keepdims=True
    )
    window_weights = (window_exp / denominator).astype(jnp.bfloat16)
    context_weights = (context_exp / denominator).astype(jnp.bfloat16)
    attended = jnp.einsum(
        "rbhqk,rbkhd->rbqhd", window_weights, window_values, preferred_element_type=jnp.float32
    )
    attended = attended + jnp.einsum(
        "rbhqk,khd->rbqhd", context_weights, context_values, preferred_element_type=jnp.float32
    )
    attended = attended.reshape(tokens, local_cols)
    gated_heads = (jax.nn.silu(silu_gate.astype(jnp.float32)) * attended).astype(jnp.bfloat16)
    out_rows = tokens // lax.axis_size("tp")
    branch = lax.psum_scatter(
        product(gated_heads, w_out).astype(jnp.bfloat16), "tp", scatter_dimension=0, tiled=True
    )
    own_rows = lax.dynamic_slice_in_dim(latent, tp_index * out_rows, out_rows, 0)
    updated = own_rows.astype(jnp.float32) + gating[0] * normalize(branch, gain_post)
    return updated.astype(jnp.bfloat16)


def low_half(shape):
    return lax.broadcasted_iota(jnp.int32, shape, len(shape) - 1) < HALF


def swap_halves(block):
    return pltpu.roll(block, HALF, len(block.shape) - 1)


def head_pair(first, second):
    low = low_half(first.shape)
    return (
        jnp.where(low, first, swap_halves(second)),
        jnp.where(low, swap_halves(first), second),
    )


def partial_kernel(
    condition_ref, context_ref, shift_ref, scale_ref, gate_ref, out_ref, active_ref
):
    rows = shift_ref.shape[0] // LANES
    for kind, source in enumerate((condition_ref, context_ref)):
        values = source[...].astype(jnp.float32)
        active_ref[kind] = values / (1.0 + jnp.exp(-values))
    own = pl.ds(lax.axis_index("sp") * rows, rows)
    vectors = [active_ref[kind, own, :].astype(jnp.bfloat16) for kind in range(2)]
    width = shift_ref.shape[1] // LANES
    row = 0
    for weight_ref, kinds in ((shift_ref, 2), (scale_ref, 2), (gate_ref, 1)):
        both = sum(
            jnp.dot(
                jnp.concatenate([vectors[kind][part : part + 1] for kind in range(2)], axis=0),
                weight_ref[part * LANES : (part + 1) * LANES, :],
                preferred_element_type=jnp.float32,
            )
            for part in range(rows)
        )
        for kind in range(kinds):
            for lane in range(width):
                block = both[kind : kind + 1, lane * LANES : (lane + 1) * LANES].astype(out_ref.dtype)
                out_ref[:, row : row + 1, :] = jnp.broadcast_to(block[None], (out_ref.shape[0], 1, LANES))
                row += 1


def norms(values):
    mean = jnp.sum(values * values, axis=-1, keepdims=True) * (1.0 / values.shape[-1])
    return lax.rsqrt(mean + EPSILON)


def norm_kernel(
    latent_ref, before_ref, after_ref, context_hbm, out_ref, before_out, after_out, half_ref, semaphore
):
    count = half_ref.shape[0]
    first = pl.multiple_of(lax.axis_index("tp") % 2 * count, count)
    copy = pltpu.make_async_copy(context_hbm.at[pl.ds(first, count)], half_ref, semaphore)
    copy.start()
    before_out[...] = jnp.broadcast_to(before_ref[...], before_out.shape)
    after_out[...] = jnp.broadcast_to(after_ref[...], after_out.shape)
    step = 32

    def body(index, carry):
        rows = pl.ds(pl.multiple_of(index * step, step), step)
        norm = norms(latent_ref[rows, :].astype(jnp.float32))
        out_ref[rows, :] = jnp.broadcast_to(norm, (step, LANES))
        return carry

    lax.fori_loop(0, latent_ref.shape[0] // step, body, 0)
    copy.wait()


def modulate_rows(source, target, first, count, vectors_ref, gain_ref, kind, norm_ref=None):
    factor = gain_ref[:1, :] * (1.0 + vectors_ref[2 + kind : 3 + kind, :])
    shift = vectors_ref[kind : kind + 1, :]
    step = 32

    def body(index, carry):
        start = pl.multiple_of(index * step, step)
        values = source[pl.ds(start, step), :].astype(jnp.float32)
        norm = norms(values) if norm_ref is None else norm_ref[pl.ds(start, step), :][:, :1]
        target[pl.ds(pl.multiple_of(first + start, step), step), :] = (
            values * norm * factor + shift
        ).astype(jnp.bfloat16)
        return carry

    lax.fori_loop(0, count // step, body, 0)


def start_all(pairs, semaphores):
    copies = [
        pltpu.make_async_copy(source, target, semaphores.at[index])
        for index, (source, target) in enumerate(pairs)
    ]
    for copy in copies:
        copy.start()
    return copies


def project_kernel(
    terms_ref, latent_hbm, norm_hbm, gain_hbm, key_hbm, value_hbm, query_hbm,
    send_hbm, hidden_hbm, vectors_hbm,
    latent_ref, norm_ref, gain_ref, key_ref, value_ref, query_ref,
    send_ref, hidden_ref, vectors_ref, loads, stores,
    *, sp_count, tp_count
):
    copies = start_all(
        (
            (norm_hbm, norm_ref),
            (gain_hbm, gain_ref),
            (latent_hbm, latent_ref),
            (key_hbm, key_ref),
            (value_hbm, value_ref),
            (query_hbm, query_ref),
        ),
        loads,
    )
    saves = []

    def save(source, target):
        saves.append(pltpu.make_async_copy(source, target, stores.at[len(saves)]))
        saves[-1].start()

    cols = key_ref.shape[1]
    width = cols // LANES
    for part in range(tp_count):
        total = terms_ref[part].astype(jnp.float32)
        for other in range(1, sp_count):
            total = total + terms_ref[other * tp_count + part].astype(jnp.float32)
        for index in range(5):
            for lane in range(width):
                first = part * cols + lane * LANES
                row = index * width + lane
                vectors_ref[index : index + 1, first : first + LANES] = total[row : row + 1]
    vectors_ref[5:, :] = jnp.zeros((vectors_ref.shape[0] - 5, vectors_ref.shape[1]), jnp.float32)
    save(vectors_ref, vectors_hbm)
    tokens = latent_ref.shape[0]
    half = tokens // 2
    for copy in copies[:3]:
        copy.wait()
    modulate_rows(latent_ref, hidden_ref, 0, tokens, vectors_ref, gain_ref, 0, norm_ref)
    save(hidden_ref, hidden_hbm)
    copies[3].wait()
    keys = jnp.dot(hidden_ref[...], key_ref[...], preferred_element_type=jnp.float32)
    copies[4].wait()
    values = jnp.dot(hidden_ref[...], value_ref[...], preferred_element_type=jnp.float32)
    for pair in range(width):
        lanes = slice(pair * LANES, (pair + 1) * LANES)
        for head, kv in enumerate(head_pair(keys[:, lanes], values[:, lanes])):
            send_ref[2 * pair + head, :tokens, :] = kv.astype(jnp.bfloat16)
    save(send_ref.at[:, pl.ds(0, tokens)], send_hbm.at[:, pl.ds(0, tokens)])
    copies[5].wait()
    queries = jnp.dot(hidden_ref[...], query_ref[...], preferred_element_type=jnp.float32)
    for pair in range(width):
        lanes = slice(pair * LANES, (pair + 1) * LANES)
        block = queries[:, lanes].astype(jnp.bfloat16).astype(jnp.float32) * HALF**-0.5
        for head, packed in enumerate(head_pair(block[:half], block[half:])):
            send_ref[2 * pair + head, tokens:, :] = packed.astype(jnp.bfloat16)
    save(send_ref.at[:, pl.ds(tokens, half)], send_hbm.at[:, pl.ds(tokens, half)])
    for copy in saves:
        copy.wait()


def context_kernel(*refs, sp_count, sources, copied):
    heads = sp_count // 2
    source_refs, (vectors_hbm, gain_hbm, key_hbm, value_hbm) = refs[:sources], refs[sources : sources + 4]
    outs, refs = refs[sources + 4 : sources + 4 + heads], refs[sources + 4 + heads :]
    (vectors_ref, gain_ref, key_ref, value_ref, hidden_ref, send_ref, loads, stores, *rows_refs) = refs
    own = lax.axis_index("sp")
    width = key_ref.shape[1]
    cols = pl.ds(pl.multiple_of(own // heads * width, width), width)
    copies = start_all(
        (
            (vectors_hbm, vectors_ref),
            (gain_hbm, gain_ref),
            *(zip(source_refs, rows_refs) if copied else ()),
            (key_hbm.at[:, cols], key_ref),
            (value_hbm.at[:, cols], value_ref),
        ),
        loads,
    )
    for copy in copies[:-2]:
        copy.wait()
    first = 0
    for source in rows_refs if copied else source_refs:
        modulate_rows(source, hidden_ref, first, source.shape[0], vectors_ref, gain_ref, 1)
        first += source.shape[0]
    copies[-2].wait()
    keys = jnp.dot(hidden_ref[...], key_ref[...], preferred_element_type=jnp.float32)
    copies[-1].wait()
    values = jnp.dot(hidden_ref[...], value_ref[...], preferred_element_type=jnp.float32)
    for pair in range(heads // 2):
        lanes = slice(pair * LANES, (pair + 1) * LANES)
        for head, kv in enumerate(head_pair(keys[:, lanes], values[:, lanes])):
            send_ref[2 * pair + head] = kv.astype(jnp.bfloat16)
    for copy in start_all(
        [(send_ref.at[own % heads ^ offset], out) for offset, out in enumerate(outs)], stores
    ):
        copy.wait()


def gate_kernel(hidden_ref, weight_ref, *out_refs):
    *out_refs, rows_ref = out_refs
    rows_ref[...] = jnp.dot(hidden_ref[...], weight_ref[...], preferred_element_type=jnp.float32)
    for offset, out_ref in enumerate(out_refs):
        count = out_ref.shape[0]
        first = pl.multiple_of((lax.axis_index("tp") ^ offset) * count, count)
        out_ref[...] = rows_ref[pl.ds(first, count), :].astype(jnp.bfloat16)


def bias_kernel(table_ref, pairs_ref, rows_ref):
    rows_ref[...] = jnp.zeros_like(rows_ref)
    own = pl.ds(lax.axis_index("sp"), 1)
    for index in range(table_ref.shape[0]):
        rows_ref[index : index + 1, : table_ref.shape[2]] = table_ref[index, own, :]
    column = lax.broadcasted_iota(jnp.int32, (GRID_W, LANES), 0)
    key_column = lax.broadcasted_iota(jnp.int32, (GRID_W, LANES), 1) % GRID_W
    first_column = jnp.clip(column - WIN_COLS // 2, 0, GRID_W - WIN_COLS)
    inside = (key_column >= first_column) & (key_column < first_column + WIN_COLS)
    count = pairs_ref.shape[0]
    first = pltpu.roll(rows_ref[...], LANES - WIN_COLS + 1, 1)
    second = pltpu.roll(rows_ref[...], HALF - WIN_COLS + 1, 1)
    for index in range(count):
        row = first[index : index + 1] + second[index + 1 : index + 2]
        toeplitz = pltpu.roll(jnp.broadcast_to(row, (GRID_W, LANES)), 0, 1, stride=1, stride_axis=0)
        pairs_ref[index] = jnp.where(inside, toeplitz, HIDDEN_SCORE)


def fill_bias(bias_ref, pairs_ref, block, blocks):
    tokens, band = bias_ref.shape
    grid_rows, band_rows = tokens // GRID_W, band // GRID_W
    total_rows = blocks * grid_rows
    hidden = jnp.full((GRID_W, LANES), HIDDEN_SCORE, jnp.float32)
    low = low_half(hidden.shape)
    last = pairs_ref.shape[0] - 1
    band_first = min(max(block * grid_rows - WIN_ROWS // 2, 0), total_rows - band_rows)
    for query in range(grid_rows):
        query_row = block * grid_rows + query
        window_first = min(max(query_row - WIN_ROWS // 2, 0), total_rows - WIN_ROWS)
        for pair in range(band_rows // 2):
            key_row = band_first + 2 * pair
            valid = [window_first <= key_row + side < window_first + WIN_ROWS for side in range(2)]
            offset = key_row - query_row + WIN_ROWS - 1
            if not any(valid):
                tile = hidden
            elif 0 <= offset <= last:
                tile = pairs_ref[offset]
            else:
                tile = swap_halves(pairs_ref[last if offset > last else 0])
            if any(valid) and not all(valid):
                tile = jnp.where(low if valid[0] else ~low, tile, hidden)
            bias_ref[
                query * GRID_W : (query + 1) * GRID_W, pair * LANES : (pair + 1) * LANES
            ] = tile


def with_ones(kv):
    return jnp.where(low_half(kv.shape), jnp.ones_like(kv), kv)


CONTRACT_LANES = (((1,), (1,)), ((), ()))


def attend_kernel(received_ref, *refs):
    *sources, pairs_hbm, out_hbm = refs[:-8]
    pairs_ref, out_ref, ones_ref, context_ref, context_ones_ref, query_ref, bias_ref, semaphores = refs[-8:]
    blocks = received_ref.shape[0]
    tokens = query_ref.shape[1]
    rows = context_ref.shape[0] // len(sources)
    loads = start_all([(pairs_hbm, pairs_ref)], semaphores)
    for index, source in enumerate(sources):
        kv = source[...]
        context_ref[index * rows : (index + 1) * rows, :] = kv
        context_ones_ref[index * rows : (index + 1) * rows, :] = with_ones(kv)
    parts = out_ref.shape[0] // blocks
    chunk = tokens // parts
    half = tokens // 2
    for block in range(blocks):
        ones_ref[block * tokens : (block + 1) * tokens, :] = with_ones(received_ref[block, :tokens, :])
        packed = received_ref[block, tokens:, :].astype(jnp.float32)
        low = low_half(packed.shape)
        query_ref[block, :half, :] = jnp.where(low, packed, 0.0).astype(jnp.bfloat16)
        query_ref[block, half:, :] = jnp.where(low, swap_halves(packed), 0.0).astype(jnp.bfloat16)
    low = low_half((chunk // 2, LANES))
    saves = []
    for block in range(blocks):
        band = min(max(block - 1, 0), blocks - 3)
        queries = query_ref[block]
        context = lax.dot_general(
            queries, context_ref[...], CONTRACT_LANES, preferred_element_type=jnp.float32
        )
        if block == 0:
            for load in loads:
                load.wait()
        if block in (0, 1, blocks - 1):
            fill_bias(bias_ref, pairs_ref, block, blocks)
        window = jnp.concatenate(
            [
                lax.dot_general(
                    queries,
                    received_ref[band + part, :tokens, :],
                    CONTRACT_LANES,
                    preferred_element_type=jnp.float32,
                )
                for part in range(3)
            ],
            axis=1,
        ) + bias_ref[...]
        maximum = jnp.maximum(
            jnp.max(window, axis=-1, keepdims=True), jnp.max(context, axis=-1, keepdims=True)
        )
        sums = jnp.dot(
            jnp.exp(context - maximum).astype(jnp.bfloat16),
            context_ones_ref[...],
            preferred_element_type=jnp.float32,
        ) + jnp.dot(
            jnp.exp(window - maximum).astype(jnp.bfloat16),
            ones_ref[band * tokens : (band + 3) * tokens, :],
            preferred_element_type=jnp.float32,
        )
        attended = sums / swap_halves(sums)
        for part in range(parts):
            rows = attended[part * chunk : (part + 1) * chunk]
            out_ref[block * parts + part] = jnp.where(
                low, swap_halves(rows[: chunk // 2]), rows[chunk // 2 :]
            ).astype(jnp.bfloat16)
        own = pl.ds(block * parts, parts)
        saves.append(pltpu.make_async_copy(out_ref.at[own], out_hbm.at[own], semaphores.at[block]))
        saves[-1].start()
    for save in saves:
        save.wait()


def output_kernel(attended_ref, own_weight_ref, *refs, sp_count, tp_count):
    small = 3
    gate_refs, refs = refs[:tp_count], refs[tp_count:]
    sources, refs = refs[:small], refs[small:]
    weights, refs = refs[: tp_count - 1], refs[tp_count - 1 :]
    out_ref, gated_ref, weight_ref, *targets, semaphores = refs
    count = targets[0].shape[0]
    own = pl.ds(pl.multiple_of(lax.axis_index("tp") * count, count), count)
    sources = (sources[0].at[own], *sources[1:])
    pieces = (semaphores.shape[0] - small) // (tp_count - 1)
    depth = weight_ref.shape[1] // pieces
    pairs = list(zip(sources, targets)) + [
        (source.at[rows], weight_ref.at[index, rows])
        for index, source in enumerate(weights)
        for rows in (pl.ds(piece * depth, depth) for piece in range(pieces))
    ]
    copies = [
        pltpu.make_async_copy(source, target, semaphores.at[index])
        for index, (source, target) in enumerate(pairs)
    ]
    for copy in copies:
        copy.start()
    latent_ref, vectors_ref, gain_ref = targets
    half = attended_ref.shape[1]
    for offset in range(tp_count):
        group = lax.axis_index("tp") ^ offset
        for pair in range(sp_count // 2):
            first = attended_ref[2 * pair * tp_count + group].astype(jnp.float32)
            second = attended_ref[(2 * pair + 1) * tp_count + group].astype(jnp.float32)
            lanes = slice(pair * LANES, (pair + 1) * LANES)
            for side, block in enumerate(head_pair(first, second)):
                gate = gate_refs[offset][side * half : (side + 1) * half, lanes].astype(jnp.float32)
                gated_ref[offset, side * half : (side + 1) * half, lanes] = (
                    gate / (1.0 + jnp.exp(-gate)) * block
                ).astype(jnp.bfloat16)
    total = jnp.dot(gated_ref[0], own_weight_ref[...], preferred_element_type=jnp.float32)
    for index, copy in enumerate(copies[small:]):
        offset, piece = divmod(index, pieces)
        rows = slice(piece * depth, (piece + 1) * depth)
        copy.wait()
        total = total + jnp.dot(
            gated_ref[1 + offset, :, rows],
            weight_ref[offset, rows, :],
            preferred_element_type=jnp.float32,
        )
    for copy in copies[:small]:
        copy.wait()
    branch = total.astype(jnp.bfloat16).astype(jnp.float32)
    mean = jnp.sum(branch * branch, axis=-1, keepdims=True) * (1.0 / branch.shape[-1])
    out_ref[...] = (
        latent_ref[...].astype(jnp.float32)
        + vectors_ref[4:5, :] * (branch * lax.rsqrt(mean + EPSILON)) * gain_ref[:1, :]
    ).astype(jnp.bfloat16)


def in_vmem(array):
    return pltpu.with_memory_space_constraint(array, pltpu.VMEM)


def call(kernel, out_shape, operands, scratch=(), raw=0, raw_outs=(), flops=0, mib=58):
    vmem, hbm = pl.BlockSpec(), pl.BlockSpec(memory_space=pl.ANY)
    single = not isinstance(out_shape, tuple)
    out_specs = [
        hbm if index in raw_outs else vmem for index in range(1 if single else len(out_shape))
    ]
    return pl.pallas_call(
        kernel,
        in_specs=[vmem] * (len(operands) - raw) + [hbm] * raw,
        out_specs=out_specs[0] if single else out_specs,
        out_shape=out_shape,
        scratch_shapes=scratch,
        cost_estimate=pl.CostEstimate(flops=flops, transcendentals=0, bytes_accessed=0),
        compiler_params=pltpu.CompilerParams(vmem_limit_bytes=mib * 2**20),
    )(*operands)


def shards_by_heads(
    latent,
    context,
    condition,
    context_condition,
    gain_pre,
    gain_post,
    w_shift,
    w_scale,
    w_gate,
    w_query,
    w_key,
    w_value,
    w_silu,
    offset_bias,
    w_out,
):
    sp_count, tp_count = lax.axis_size("sp"), lax.axis_size("tp")
    cols = w_shift.shape[1]
    tokens, model_width = latent.shape
    context_tokens = context.shape[0]
    rows = tokens + tokens // 2
    width = cols // LANES
    f32, bf16 = jnp.float32, jnp.bfloat16
    vmem = pltpu.VMEM

    shape = jax.ShapeDtypeStruct
    across = [(index, index ^ (tp_count // 2)) for index in range(tp_count)]
    beside = [(index, index ^ 1) for index in range(tp_count)]
    dma = pltpu.SemaphoreType.DMA

    terms = call(
        partial_kernel,
        shape((sp_count * tp_count, 5 * width, LANES), bf16),
        (
            condition.reshape(-1, LANES),
            context_condition.reshape(-1, LANES),
            w_shift,
            w_scale,
            w_gate,
        ),
        scratch=[vmem((2, model_width // LANES, LANES), f32)],
    )
    terms = lax.all_to_all(terms, ("sp", "tp"), 0, 0, tiled=True)
    far = lax.ppermute(w_out, "tp", across)
    near = lax.ppermute(w_out, "tp", beside)
    norm, gain, gain_after, context_half = call(
        norm_kernel,
        (
            shape((tokens, LANES), f32),
            shape((8, model_width), f32),
            shape((8, model_width), f32),
            shape((context_tokens // 2, model_width), bf16),
        ),
        (latent, gain_pre.reshape(1, -1), gain_post.reshape(1, -1), context),
        raw=1,
        scratch=[dma],
        flops=3 * 10**9,
    )
    opposite = [(index, index ^ (sp_count // 2)) for index in range(sp_count)]
    far_context = lax.ppermute(context_half, "sp", opposite)
    offsets = offset_bias.shape[1]
    pairs = call(
        bias_kernel,
        shape((offsets - 1, GRID_W, LANES), f32),
        (jnp.transpose(offset_bias, (1, 0, 2)),),
        scratch=[vmem((16, LANES), f32)],
        flops=3 * 10**9,
    )
    send, hidden, vectors = call(
        functools.partial(project_kernel, sp_count=sp_count, tp_count=tp_count),
        (
            shape((sp_count, rows, LANES), bf16),
            shape((tokens, model_width), bf16),
            shape((8, model_width), f32),
        ),
        (in_vmem(terms), latent, norm, gain, w_key, w_value, w_query),
        raw=6,
        raw_outs=(0, 1, 2),
        scratch=[
            vmem(latent.shape, bf16),
            vmem(norm.shape, f32),
            vmem((8, model_width), f32),
            vmem(w_key.shape, bf16),
            vmem(w_value.shape, bf16),
            vmem(w_query.shape, bf16),
            vmem((sp_count, rows, LANES), bf16),
            vmem(latent.shape, bf16),
            vmem((8, model_width), f32),
            dma((6,)),
            dma((4,)),
        ],
        flops=10**9,
    )
    received = lax.all_to_all(send, "sp", 0, 0, tiled=True)
    group = sp_count // 2

    def context_heads(*sources, copied=False):
        count = sum(source.shape[0] for source in sources)
        return call(
            functools.partial(
                context_kernel, sp_count=sp_count, sources=len(sources), copied=copied
            ),
            (shape((count, LANES), bf16),) * group,
            (*sources, vectors, gain, w_key, w_value),
            raw=4 + copied * len(sources),
            raw_outs=tuple(range(group)),
            scratch=[
                vmem((8, model_width), f32),
                vmem((8, model_width), f32),
                vmem((model_width, cols // 2), bf16),
                vmem((model_width, cols // 2), bf16),
                vmem((count, model_width), bf16),
                vmem((group, count, LANES), bf16),
                dma((4 + copied * len(sources),)),
                dma((group,)),
            ]
            + [vmem(source.shape, bf16) for source in sources if copied],
            flops=10**9,
        )

    def context_exchange(parts):
        return [parts[0]] + [
            lax.ppermute(
                parts[offset], "sp", [(index, index ^ offset) for index in range(sp_count)]
            )
            for offset in range(1, group)
        ]

    context_kv = context_exchange(context_heads(context, copied=True))
    near_context = lax.ppermute(far_context, "tp", beside)
    context_kv += context_exchange(context_heads(in_vmem(far_context), in_vmem(near_context)))
    out_rows = tokens // tp_count
    gates = call(
        gate_kernel,
        (shape((out_rows, cols), bf16),) * tp_count,
        (hidden, w_silu),
        scratch=[vmem((tokens, cols), f32)],
        flops=10**9,
    )
    gates = [gates[0]] + [
        lax.ppermute(gates[offset], "tp", [(index, index ^ offset) for index in range(tp_count)])
        for offset in range(1, tp_count)
    ]
    relayed = lax.ppermute(far, "tp", beside)
    attended = call(
        attend_kernel,
        shape((sp_count * tp_count, out_rows // 2, LANES), bf16),
        (in_vmem(received), *map(in_vmem, context_kv), pairs),
        raw=1,
        raw_outs=(0,),
        scratch=[
            vmem(pairs.shape, f32),
            vmem((sp_count * tp_count, out_rows // 2, LANES), bf16),
            vmem((sp_count * tokens, LANES), bf16),
            vmem((sp_count * context_tokens, LANES), bf16),
            vmem((sp_count * context_tokens, LANES), bf16),
            vmem((sp_count, tokens, LANES), bf16),
            vmem((tokens, 3 * tokens), f32),
            dma((sp_count,)),
        ],
        flops=5 * 10**9,
    )
    attended = lax.all_to_all(attended, ("sp", "tp"), 0, 0, tiled=True)
    return call(
        functools.partial(output_kernel, sp_count=sp_count, tp_count=tp_count),
        shape((out_rows, model_width), bf16),
        (
            in_vmem(attended),
            in_vmem(w_out),
            *map(in_vmem, gates),
            latent,
            vectors,
            gain_after,
            near,
            far,
            relayed,
        ),
        scratch=[
            vmem((tp_count, out_rows, cols), bf16),
            vmem((tp_count - 1, cols, model_width), bf16),
            vmem((out_rows, model_width), bf16),
            vmem((8, model_width), f32),
            vmem((8, model_width), f32),
            dma((2 * tp_count + 1,)),
        ],
        raw=tp_count + 2,
        flops=10**9,
    )


def solution(mesh):
    in_specs = (
        P("sp", None),
        P("sp", None),
        P(),
        P(),
        P(),
        P(),
        P("sp", "tp"),
        P("sp", "tp"),
        P("sp", "tp"),
        P(None, "tp"),
        P(None, "tp"),
        P(None, "tp"),
        P(None, "tp"),
        P("tp", None, None),
        P("tp", None),
    )
    out_specs = P(("sp", "tp"), None)
    sp_count, tp_count = mesh.shape["sp"], mesh.shape["tp"]

    def shards(*arrays):
        heads = arrays[13].shape[0]
        head_width = arrays[6].shape[1] // heads
        grid_rows = arrays[0].shape[0] // GRID_W
        one_head_each = (
            heads == sp_count
            and tp_count == 4
            and sp_count == 8
            and head_width == HALF
            and GRID_W == HALF
            and 2 * grid_rows == WIN_ROWS
        )
        return (shards_by_heads if one_head_each else shards_by_rows)(*arrays)

    return jax.shard_map(shards, mesh=mesh, in_specs=in_specs, out_specs=out_specs, check_vma=False)
```
